128 devices in a mesh: sp: 16 (over z, x), tp: 8 (over y, core).
Axes of the slice: x: 4, y: 4, z: 4, core: 2. Of those that a mesh axis runs over, the one named last changes fastest.
Arguments:
- tokens: bfloat16 [2048, 1024], P('sp', 'tp'), may hold values from -6 to 6
- norm_gain: float32 [3, 1024], replicated, may hold values from 0.1 to 1.9
- w_query: bfloat16 [3, 1024, 1024], P(None, 'sp', 'tp'), may hold values from -0.1875 to 0.1875
- w_key: bfloat16 [3, 1024, 1024], P(None, 'sp', 'tp'), may hold values from -0.1875 to 0.1875
- w_value: bfloat16 [3, 1024, 1024], P(None, 'sp', 'tp'), may hold values from -0.1875 to 0.1875
- w_out: bfloat16 [3, 1024, 1024], P(None, 'tp', 'sp'), may hold values from -0.5625 to 0.5625
- offset_bias: float32 [3, 16, 8, 16], P(None, 'tp'), may hold values from -3 to 3
- documents: int32 [2048], P('sp'), may hold values from 0 to 15, never falling along the last dimension, each value on 1 to 256 neighbouring positions
Outputs:
- mixed: bfloat16 [2048, 1024], P('sp', 'tp')
The draws below stay inside these ranges and needn't reach their ends.
Inputs may be any that keep to these rules, and one draw needn't show every extreme that they name: `documents`: document numbers never fall along the token order, start at 0, and each document has 1 to 256 tokens.
All inputs are finite; a program needn't handle non-finite values.
Results may differ from the reference program's by a relative error of at most 0.02.
Values may be sent and summed in bfloat16 or wider, within the bound.
A program may use at most 64 MiB of HBM per device.

```python
import math
import jax
import jax.numpy as jnp
import numpy as np
from jax import lax

HEADS = 16
HEAD_DIM = 64
D = 1024
WIN_ROWS = 8
WIN_COLS = 16
LAYERS = 3
ROWS_DEV = 4
GRID_W = 32
TOKENS = 2048


def level_of(own_key, dims, pieces, low, largest):
    factor_of = 1.0
    for dim, blocks in pieces:
        heights = jax.random.uniform(jax.random.fold_in(jax.random.fold_in(own_key, 6), dim), (blocks,), jnp.float32, low / len(pieces), largest / len(pieces))
        factor_of = factor_of * jnp.repeat(jnp.exp(heights), dims[dim] // blocks).reshape((-1,) + (1,) * (len(dims) - 1 - dim))
    return factor_of


def length_profile(number_of, total, most, slope):
    weights = [(1 << 20) // math.isqrt(grade ** slope) + 1 for grade in range(2, number_of + 1)]
    spare, given = total - most - (number_of - 1), [1] * (number_of - 1)
    while spare > 0:
        movable = [i for i in range(number_of - 1) if given[i] < most]
        whole, left = sum([weights[i] for i in movable]), spare
        for i in movable:
            more = min(most - given[i], max(1, left * weights[i] // whole), spare)
            given[i] = given[i] + more
            spare = spare - more
    return np.array([most] + given)


def uneven_parts(own_key, count, total, most, skew):
    if count == 2:
        one = jax.random.randint(own_key, (), max(1, total - most), min(most, total - 1) + 1)
        return jnp.stack([one, total - one])
    lengths = jnp.asarray(length_profile(count, total, most, skew), jnp.int32)
    pairs = (count - 1) // 2
    giver, sink = lengths[1:1 + 2 * pairs:2], lengths[2:2 + 2 * pairs:2]
    margin = jnp.minimum(giver - 1, most - sink)
    shifted = jax.random.randint(jax.random.fold_in(own_key, 1), (pairs,), 0, 1 << 20) % (margin + 1)
    lengths = lengths.at[1:1 + 2 * pairs:2].set(giver - shifted).at[2:2 + 2 * pairs:2].set(sink + shifted)
    return lengths[jax.random.permutation(jax.random.fold_in(own_key, 2), count)]


def centred(stream_key, shape, deviation, bound, split=(), held_as=jnp.bfloat16):
    result = deviation * jax.random.normal(stream_key, shape, jnp.float32)
    if split:
        result = result * level_of(stream_key, shape, split, -0.22, 0.18)
    return jnp.clip(result, -bound, bound).astype(held_as)


def setup_inputs(seed: int = 0) -> dict:
    keys = jax.random.split(jax.random.key(seed), 9)
    return {
        "tokens": centred(keys[0], (TOKENS, D), 1.0, 6.0, ((0, 16), (1, 8))),
        "norm_gain": jnp.clip(1.0 + 0.18 * jax.random.normal(keys[1], (LAYERS, D), jnp.float32), 0.1, 1.9),
        "w_query": centred(keys[2], (LAYERS, D, D), D ** -0.5, 0.1875, ((1, 16), (2, 8))),
        "w_key": centred(keys[3], (LAYERS, D, D), D ** -0.5, 0.1875, ((1, 16), (2, 8))),
        "w_value": centred(keys[4], (LAYERS, D, D), D ** -0.5, 0.1875, ((1, 16), (2, 8))),
        "w_out": centred(keys[5], (LAYERS, D, D), (3.0 / D ** 0.5), 0.5625, ((1, 8), (2, 16))),
        "offset_bias": centred(keys[6], (LAYERS, HEADS, WIN_ROWS, WIN_COLS), 0.5, 3.0, ((1, 8),), jnp.float32),
        "documents": jnp.searchsorted(jnp.cumsum(uneven_parts(keys[7], TOKENS // (ROWS_DEV * GRID_W), TOKENS, 2 * ROWS_DEV * GRID_W, 2)), jnp.arange(TOKENS), side="right").astype(jnp.int32),
    }


EPS = 1e-06

def rms_rows(stream, gain_row):
    values = stream.astype(jnp.float32)
    mean_sq = lax.optimization_barrier(jnp.mean(values * values, axis=-1, keepdims=True))
    return (values * lax.rsqrt(mean_sq + EPS) * gain_row).astype(jnp.bfloat16)

def head_norm(heads_raw):
    values = heads_raw.astype(jnp.float32)
    mean_sq = lax.optimization_barrier(jnp.mean(values * values, axis=-1, keepdims=True))
    return (values * lax.rsqrt(mean_sq + EPS)).astype(jnp.bfloat16)

def attend(queries, fringe, seg_own, seg_fringe, bias_layer):
    row_count, grid_width, head_count, head_width = queries.shape
    key_rows = jnp.stack([fringe[row_lag:row_lag + row_count] for row_lag in range(WIN_ROWS)], axis=1)
    seg_rows = jnp.stack([seg_fringe[row_lag:row_lag + row_count] for row_lag in range(WIN_ROWS)], axis=1)
    key_part = key_rows[..., :head_width].astype(jnp.float32)
    value_part = key_rows[..., head_width:].astype(jnp.float32)
    scores = jnp.einsum('rchd,rjkhd->rhcjk', queries.astype(jnp.float32), key_part) * head_width ** (-0.5)
    column = jnp.arange(grid_width)
    col_offset = column[None, :] - column[:, None] + WIN_COLS // 2
    inside = (col_offset >= 0) & (col_offset < WIN_COLS)
    bias_table = bias_layer[:, :, jnp.clip(col_offset, 0, WIN_COLS - 1)]
    scores = scores + jnp.transpose(bias_table, (0, 2, 1, 3))[None]
    same_doc = seg_rows[:, None, None, :, :] == seg_own[:, None, :, None, None]
    allowed = same_doc & inside[None, None, :, None, :]
    scores = jnp.where(allowed, scores, -1e+30)
    flat = scores.reshape(row_count, head_count, grid_width, WIN_ROWS * grid_width)
    attn_probs = jax.nn.softmax(flat, axis=-1).astype(jnp.bfloat16)
    attn_probs = attn_probs.reshape(row_count, head_count, grid_width, WIN_ROWS, grid_width)
    mixed_heads = jnp.einsum('rhcjk,rjkhd->rchd', attn_probs.astype(jnp.float32), value_part)
    return mixed_heads.astype(jnp.bfloat16)

def reference(tokens, norm_gain, w_query, w_key, w_value, w_out, offset_bias, documents):
    row_count = TOKENS // GRID_W
    reach_rows = WIN_ROWS // 2
    seg_own = (documents + 1).reshape(row_count, GRID_W)
    seg_fringe = jnp.pad(seg_own, ((reach_rows, reach_rows), (0, 0)))
    stream = tokens
    for layer_index in range(LAYERS):
        normed = rms_rows(stream, norm_gain[layer_index])
        query_raw = jnp.dot(normed, w_query[layer_index], preferred_element_type=jnp.float32).astype(jnp.bfloat16)
        key_raw = jnp.dot(normed, w_key[layer_index], preferred_element_type=jnp.float32).astype(jnp.bfloat16)
        value_heads = jnp.dot(normed, w_value[layer_index], preferred_element_type=jnp.float32).astype(jnp.bfloat16)
        query_heads = head_norm(query_raw.reshape(row_count, GRID_W, HEADS, HEAD_DIM))
        key_heads = head_norm(key_raw.reshape(row_count, GRID_W, HEADS, HEAD_DIM))
        value_heads = value_heads.reshape(row_count, GRID_W, HEADS, HEAD_DIM)
        key_value = jnp.concatenate([key_heads, value_heads], axis=-1)
        fringe = jnp.pad(key_value, ((reach_rows, reach_rows), (0, 0), (0, 0), (0, 0)))
        attended = attend(query_heads, fringe, seg_own, seg_fringe, offset_bias[layer_index])
        attended = attended.reshape(TOKENS, HEADS * HEAD_DIM)
        stream = jnp.dot(attended, w_out[layer_index], preferred_element_type=jnp.float32).astype(jnp.bfloat16)
    return stream
```

```python
import jax
import jax.numpy as jnp
from jax import lax
from jax.experimental import pallas as pl
from jax.experimental.pallas import tpu as pltpu
from jax.sharding import PartitionSpec as P

MESH = pl.DeviceIdType.MESH
LAYERS = 3
EPS = 1e-06
NEG = -1e30
BF = jnp.bfloat16
F32 = jnp.float32

RING = (2, 1, 3)
TP_PEERS = ((2, 0), (2, 1), (1, 0), (3, 0), (1, 1), (3, 1), (0, 1))

N_AG = 7
N_W = 12
N_HALO = 2
N_RS = 7
AG0 = 0
W0 = AG0 + LAYERS * N_AG
HALO0 = W0 + LAYERS * N_W
RS0 = HALO0 + LAYERS * N_HALO
DOC0 = RS0 + LAYERS * N_RS
N_COPIES = DOC0 + 2


def kernel(
    tok_ref, gain_ref, wq_ref, wk_ref, wv_ref, wo_ref, bias_ref, docs_ref, out_ref,
    W, G, KV, DOC, R, S, BM, PB, ssem, rsem, lsem,
):
    s = lax.axis_index("sp")
    t = lax.axis_index("tp")
    z, x = s // 4, s % 4
    y, c = t // 2, t % 2
    sends = []

    def rdma(src, dst, sem, device):
        copy = pltpu.make_async_remote_copy(
            src_ref=src,
            dst_ref=dst,
            send_sem=ssem.at[sem],
            recv_sem=rsem.at[sem],
            device_id=device,
            device_id_type=MESH,
        )
        copy.start()
        sends.append(copy)
        return copy

    def tp_peer(dy, dc):
        return ((y + dy) % 4) * 2 + (c + dc) % 2

    local = [
        pltpu.make_async_copy(tok_ref, G.at[0, t], lsem.at[0]),
        pltpu.make_async_copy(docs_ref, DOC.at[1], lsem.at[1]),
        pltpu.make_async_copy(wq_ref, W.at[:, 0, z, x], lsem.at[2]),
        pltpu.make_async_copy(wk_ref, W.at[:, 1, z, x], lsem.at[3]),
        pltpu.make_async_copy(wv_ref, W.at[:, 2, z, x], lsem.at[4]),
    ]
    for copy in local:
        copy.start()

    barrier = pltpu.get_barrier_semaphore()
    for k in range(1, 16):
        pl.semaphore_signal(barrier, inc=1, device_id={"sp": (s + k) % 16}, device_id_type=MESH)
    for k in range(1, 8):
        pl.semaphore_signal(barrier, inc=1, device_id={"tp": (t + k) % 8}, device_id_type=MESH)

    for l in range(LAYERS):
        W[l, 3, z, x] = wo_ref[l].astype(F32).T.astype(BF)
    PB[...] = jnp.zeros_like(PB)

    for copy in local:
        copy.wait()
    pl.semaphore_wait(barrier, 22)

    def gather_tp(l):
        return [
            rdma(G.at[l, t], G.at[l, t], AG0 + l * N_AG + i, {"tp": tp_peer(dy, dc)})
            for i, (dy, dc) in enumerate(TP_PEERS)
        ]

    nxt, prv = (s + 1) % 16, (s + 15) % 16
    gathers = gather_tp(0)
    doc_copies = [
        rdma(DOC.at[1], DOC.at[0], DOC0, {"sp": nxt}),
        rdma(DOC.at[1], DOC.at[2], DOC0 + 1, {"sp": prv}),
    ]

    def phase_one(l):
        base = W0 + l * N_W
        along_x = [
            rdma(W.at[l, 0:2, z, x], W.at[l, 0:2, z, x], base + i, {"sp": z * 4 + (x + d) % 4})
            for i, d in enumerate(RING)
        ]
        along_z = [
            rdma(W.at[l, 2:4, z, x], W.at[l, 2:4, z, x], base + 3 + i, {"sp": ((z + d) % 4) * 4 + x})
            for i, d in enumerate(RING)
        ]
        return along_x, along_z

    def phase_two(l, first):
        base = W0 + l * N_W + 6
        along_x, along_z = first
        for copy in along_x:
            copy.wait_recv()
        then_z = [
            rdma(W.at[l, 0:2, z], W.at[l, 0:2, z], base + i, {"sp": ((z + d) % 4) * 4 + x})
            for i, d in enumerate(RING)
        ]
        for copy in along_z:
            copy.wait_recv()
        then_x = [
            rdma(W.at[l, 2:4, :, x], W.at[l, 2:4, :, x], base + 3 + i, {"sp": z * 4 + (x + d) % 4})
            for i, d in enumerate(RING)
        ]
        return then_z + then_x

    firsts = [phase_one(l) for l in range(LAYERS)]
    weights = [phase_two(l, firsts[l]) for l in range(LAYERS)]

    for copy in doc_copies:
        copy.wait_recv()
    qi = lax.broadcasted_iota(jnp.int32, (128, 384), 0)
    kj = lax.broadcasted_iota(jnp.int32, (128, 384), 1)
    row_off = (kj >> 5) - (qi >> 5)
    col_off = (kj & 31) - (qi & 31) + 8
    key_docs = jnp.concatenate([DOC[0], DOC[1], DOC[2]], axis=1)
    eye = lax.broadcasted_iota(jnp.int32, (128, 128), 0) == lax.broadcasted_iota(jnp.int32, (128, 128), 1)
    own_docs = jnp.sum(
        jnp.where(eye, jnp.broadcast_to(DOC[1], (128, 128)).astype(F32), 0.0), axis=1, keepdims=True
    )
    lowest = jnp.where(s > 0, 0, 128)
    highest = jnp.where(s < 15, 384, 256)
    allowed = (
        (row_off >= 0) & (row_off < 8) & (col_off >= 0) & (col_off < 16)
        & (key_docs.astype(F32) == own_docs) & (kj >= lowest) & (kj < highest)
    )
    lines = jnp.zeros((6, 512), F32)
    for a in range(8):
        PB[:, 0:16] = bias_ref[:, a, :]
        lines += pltpu.roll(PB[...], 119 + 32 * a, 1)
    for l in range(LAYERS):
        for h in range(2):
            line = jnp.broadcast_to(lines[l * 2 + h : l * 2 + h + 1], (128, 512))
            table = pltpu.roll(line, 385, 1, stride=1, stride_axis=0)
            BM[l, pl.ds(h * 128, 128), :] = jnp.where(allowed, table[:, :384], NEG)

    lane = lax.broadcasted_iota(jnp.int32, (128, 128), 1)
    left = lane < 64

    def head_norm(raw):
        values = raw.astype(BF).astype(F32)
        squares = values * values
        total0 = jnp.sum(jnp.where(left, squares, 0.0), axis=1, keepdims=True)
        total1 = jnp.sum(jnp.where(left, 0.0, squares), axis=1, keepdims=True)
        mean = jnp.where(left, total0, total1) * (1.0 / 64)
        return values * lax.rsqrt(mean + EPS)

    for l in range(LAYERS):
        for copy in gathers:
            copy.wait_recv()
        total = jnp.zeros((128, 1), F32)
        for i in range(8):
            part = G[l, i].astype(F32)
            total += jnp.sum(part * part, axis=1, keepdims=True)
        scale = lax.rsqrt(total * (1.0 / 1024) + EPS)
        normed = jnp.concatenate(
            [
                (G[l, i].astype(F32) * scale * gain_ref[l : l + 1, i * 128 : (i + 1) * 128]).astype(BF)
                for i in range(8)
            ],
            axis=1,
        )
        for copy in weights[l]:
            copy.wait_recv()
        wk = W[l, 1].reshape(1024, 128)
        wv = W[l, 2].reshape(1024, 128)
        key_raw = jnp.dot(normed, wk, preferred_element_type=F32)
        value_raw = jnp.dot(normed, wv, preferred_element_type=F32)
        KV[l, 1, 0] = head_norm(key_raw).astype(BF)
        KV[l, 1, 1] = value_raw.astype(BF)
        halos = [
            rdma(KV.at[l, 1], KV.at[l, 0], HALO0 + l * N_HALO, {"sp": nxt}),
            rdma(KV.at[l, 1], KV.at[l, 2], HALO0 + l * N_HALO + 1, {"sp": prv}),
        ]
        wq = W[l, 0].reshape(1024, 128)
        query = head_norm(jnp.dot(normed, wq, preferred_element_type=F32)).astype(BF)
        query = query * jnp.asarray(0.125, BF)
        zero = jnp.zeros_like(query)
        query = jnp.concatenate([jnp.where(left, query, zero), jnp.where(left, zero, query)], axis=0)
        for copy in halos:
            copy.wait_recv()
        keys = KV[l, :, 0].reshape(384, 128)
        values = KV[l, :, 1].reshape(384, 128)
        scores = lax.dot_general(
            query, keys, (((1,), (1,)), ((), ())), preferred_element_type=F32
        ) + BM[l]
        probs = jnp.exp(scores - jnp.max(scores, axis=1, keepdims=True))
        norm = jnp.sum(probs, axis=1, keepdims=True)
        mixed = jnp.dot(probs.astype(BF), values, preferred_element_type=F32) / norm
        attended = jnp.where(left, mixed[:128], mixed[128:]).astype(BF)
        partial = lax.dot_general(
            attended, W[l, 3].reshape(1024, 128), (((1,), (1,)), ((), ())), preferred_element_type=F32
        ).astype(BF)
        for i in range(8):
            S[l, i] = partial[:, i * 128 : (i + 1) * 128]
        reduces = []
        for i, (dy, dc) in enumerate(TP_PEERS):
            peer = tp_peer(dy, dc)
            reduces.append(rdma(S.at[l, peer], R.at[l, i], RS0 + l * N_RS + i, {"tp": peer}))
        result = S[l, t].astype(F32)
        for i, copy in enumerate(reduces):
            copy.wait_recv()
            result += R[l, i].astype(F32)
        if l < LAYERS - 1:
            G[l + 1, t] = result.astype(BF)
            gathers = gather_tp(l + 1)
        else:
            out_ref[...] = result.astype(BF)

    for copy in sends:
        copy.wait_send()


def local(tokens, norm_gain, w_query, w_key, w_value, w_out, offset_bias, documents):
    vmem = pl.BlockSpec(memory_space=pltpu.VMEM)
    hbm = pl.BlockSpec(memory_space=pl.ANY)
    return pl.pallas_call(
        kernel,
        out_shape=jax.ShapeDtypeStruct((128, 128), BF),
        in_specs=[hbm, vmem, hbm, hbm, hbm, vmem, vmem, hbm],
        out_specs=vmem,
        scratch_shapes=[
            pltpu.VMEM((LAYERS, 4, 4, 4, 64, 128), BF),
            pltpu.VMEM((LAYERS, 8, 128, 128), BF),
            pltpu.VMEM((LAYERS, 3, 2, 128, 128), BF),
            pltpu.VMEM((3, 1, 128), jnp.int32),
            pltpu.VMEM((LAYERS, 7, 128, 128), BF),
            pltpu.VMEM((LAYERS, 8, 128, 128), BF),
            pltpu.VMEM((LAYERS, 256, 384), F32),
            pltpu.VMEM((6, 512), F32),
            pltpu.SemaphoreType.DMA((N_COPIES,)),
            pltpu.SemaphoreType.DMA((N_COPIES,)),
            pltpu.SemaphoreType.DMA((5,)),
        ],
        compiler_params=pltpu.CompilerParams(collective_id=0, has_side_effects=True),
    )(
        tokens, norm_gain, w_query, w_key, w_value, w_out,
        offset_bias.reshape(2 * LAYERS, 8, 16), documents.reshape(1, 128),
    )


def solution(mesh):
    return jax.shard_map(
        local,
        mesh=mesh,
        in_specs=(
            P("sp", "tp"),
            P(),
            P(None, "sp", "tp"),
            P(None, "sp", "tp"),
            P(None, "sp", "tp"),
            P(None, "tp", "sp"),
            P(None, "tp", None, None),
            P("sp"),
        ),
        out_specs=P("sp", "tp"),
        check_vma=False,
    )
```

```python
import jax
import jax.numpy as jnp
from jax import lax
from jax.experimental import pallas as pl
from jax.experimental.pallas import tpu as pltpu
from jax.sharding import PartitionSpec as P

MESH = pl.DeviceIdType.MESH
LAYERS = 3
EPS = 1e-06
NEG = -1e30
BF = jnp.bfloat16
F32 = jnp.float32

RING = (2, 1, 3)
TP_PEERS = ((2, 0), (2, 1), (1, 0), (3, 0), (1, 1), (3, 1), (0, 1))
Y_FIRST = 32
N_COPIES = 160


def kernel(
    tok_ref, gain_ref, wq_ref, wk_ref, wv_ref, wo_ref, bias_ref, docs_ref, out_ref,
    W, WO, WL, G, A, KV, DOC, R, S, RX, SX, BM, PB, ssem, rsem, lsem,
):
    s = lax.axis_index("sp")
    t = lax.axis_index("tp")
    z, x = s // 4, s % 4
    y, c = t // 2, t % 2
    sends = []

    def rdma(src, dst, device):
        sem = len(sends)
        copy = pltpu.make_async_remote_copy(
            src_ref=src,
            dst_ref=dst,
            send_sem=ssem.at[sem],
            recv_sem=rsem.at[sem],
            device_id=device,
            device_id_type=MESH,
        )
        copy.start()
        sends.append(copy)
        return copy

    def arrive(name, copies):
        with jax.named_scope(name):
            for copy in copies:
                copy.wait_recv()

    def x_peer(d):
        return {"sp": z * 4 + (x + d) % 4}

    def z_peer(d):
        return {"sp": ((z + d) % 4) * 4 + x}

    def y_peer(d):
        return {"tp": ((y + d) % 4) * 2 + c}

    def tp_peer(dy, dc):
        return ((y + dy) % 4) * 2 + (c + dc) % 2

    nxt, prv = {"sp": (s + 1) % 16}, {"sp": (s + 15) % 16}
    partner = {"tp": y * 2 + 1 - c}

    local = [
        pltpu.make_async_copy(tok_ref, G.at[t], lsem.at[0]),
        pltpu.make_async_copy(docs_ref, DOC.at[1], lsem.at[1]),
        pltpu.make_async_copy(wq_ref, W.at[:, 0, z, x], lsem.at[2]),
        pltpu.make_async_copy(wk_ref, W.at[:, 1, z, x], lsem.at[3]),
        pltpu.make_async_copy(wv_ref, W.at[:, 2, z, x], lsem.at[4]),
        pltpu.make_async_copy(wo_ref.at[0:2], WO.at[:, y, z, x], lsem.at[5]),
        pltpu.make_async_copy(wo_ref.at[2], WL.at[z, x], lsem.at[6]),
    ]
    with jax.named_scope("init"):
        for copy in local:
            copy.start()

    barrier = pltpu.get_barrier_semaphore()
    greeted = [x_peer(d) for d in RING] + [z_peer(d) for d in RING] + [nxt, prv]
    greeted += [{"tp": tp_peer(dy, dc)} for dy, dc in TP_PEERS]
    for device in greeted:
        pl.semaphore_signal(barrier, inc=1, device_id=device, device_id_type=MESH)

    PB[...] = jnp.zeros_like(PB)
    for l in range(LAYERS):
        KV[l, :, 352:384, :] = jnp.zeros((2, 32, 128), BF)

    with jax.named_scope("wait_local"):
        for copy in local:
            copy.wait()
    with jax.named_scope("wait_barrier"):
        pl.semaphore_wait(barrier, len(greeted))

    def block_one(ref, rows_a, rows_b):
        along_x = [rdma(ref(z, x, rows_a), ref(z, x, rows_a), x_peer(d)) for d in RING]
        along_z = [rdma(ref(z, x, rows_b), ref(z, x, rows_b), z_peer(d)) for d in RING]
        return along_x + along_z

    def block_two(ref, rows_a, rows_b):
        every = slice(None)
        then_z = [rdma(ref(z, every, rows_a), ref(z, every, rows_a), z_peer(d)) for d in RING]
        then_x = [rdma(ref(every, x, rows_b), ref(every, x, rows_b), x_peer(d)) for d in RING]
        return then_z + then_x

    def halves(low, high):
        mid = (low + high) // 2
        return slice(low, mid), slice(mid, high)

    class Gather:
        def __init__(self, name, ref, low, high):
            self.name, self.ref, self.rows = name, ref, halves(low, high)

        def one(self):
            self.first = block_one(self.ref, *self.rows)

        def two(self):
            arrive("p1_" + self.name, self.first)
            self.second = block_two(self.ref, *self.rows)

        def done(self):
            arrive("p2_" + self.name, self.second)

    qkv = [
        Gather(f"qkv{l}", lambda i, j, rows, l=l: W.at[l, :, i, j, rows], 0, 64)
        for l in range(LAYERS)
    ]
    out_y = [
        Gather(f"oy{l}", lambda i, j, rows, l=l: WO.at[l, :, i, j, rows], 0, Y_FIRST)
        for l in range(LAYERS - 1)
    ]
    out_p = [
        Gather(f"op{l}", lambda i, j, rows, l=l: WO.at[l, y, i, j, rows], Y_FIRST, 64)
        for l in range(LAYERS - 1)
    ]
    out_last = Gather("ol", lambda i, j, rows: WL.at[i, j, rows], 0, 64)

    def cross_y_first(l):
        ref = WO.at[l, y, z, x, 0:Y_FIRST]
        return [rdma(ref, ref, y_peer(d)) for d in RING]

    def cross_y_last(l):
        ref = WO.at[l, y, :, :, Y_FIRST:64]
        return [rdma(ref, ref, y_peer(d)) for d in RING]

    gathers = [rdma(G.at[t], G.at[t], {"tp": tp_peer(dy, dc)}) for dy, dc in TP_PEERS]
    doc_copies = [rdma(DOC.at[1], DOC.at[0], nxt), rdma(DOC.at[1], DOC.at[2], prv)]
    qkv[0].one()
    crossed = [cross_y_first(l) for l in range(LAYERS - 1)]
    crossed_last = [None, None]
    out_p[0].one()

    arrive("docs", doc_copies)
    qi = lax.broadcasted_iota(jnp.int32, (128, 384), 0)
    kj = lax.broadcasted_iota(jnp.int32, (128, 384), 1)
    row_off = (kj >> 5) - (qi >> 5)
    col_off = (kj & 31) - (qi & 31) + 8
    key_docs = jnp.concatenate([DOC[0], DOC[1], DOC[2]], axis=1)
    eye = lax.broadcasted_iota(jnp.int32, (128, 128), 0) == lax.broadcasted_iota(jnp.int32, (128, 128), 1)
    own_docs = jnp.sum(
        jnp.where(eye, jnp.broadcast_to(DOC[1], (128, 128)).astype(F32), 0.0), axis=1, keepdims=True
    )
    lowest = jnp.where(s > 0, 0, 128)
    highest = jnp.where(s < 15, 384, 256)
    allowed = (
        (row_off >= 0) & (row_off < 8) & (col_off >= 0) & (col_off < 16)
        & (key_docs.astype(F32) == own_docs) & (kj >= lowest) & (kj < highest)
    )
    lines = jnp.zeros((6, 512), F32)
    for a in range(8):
        PB[:, 0:16] = bias_ref[:, a, :]
        lines += pltpu.roll(PB[...], 119 + 32 * a, 1)
    for l in range(LAYERS):
        for h in range(2):
            line = jnp.broadcast_to(lines[l * 2 + h : l * 2 + h + 1], (128, 512))
            table = pltpu.roll(line, 385, 1, stride=1, stride_axis=0)
            BM[l, pl.ds(h * 128, 128), :] = jnp.where(allowed, table[:, :384], NEG)

    lane = lax.broadcasted_iota(jnp.int32, (128, 128), 1)
    left = lane < 64

    def head_norm(raw):
        values = raw.astype(BF).astype(F32)
        squares = values * values
        total0 = jnp.sum(jnp.where(left, squares, 0.0), axis=1, keepdims=True)
        total1 = jnp.sum(jnp.where(left, 0.0, squares), axis=1, keepdims=True)
        mean = jnp.where(left, total0, total1) * (1.0 / 64)
        return values * lax.rsqrt(mean + EPS)

    qkv[0].two()
    arrive("cross0", crossed[0])
    out_y[0].one()

    for l in range(LAYERS):
        if l == 0:
            arrive("gather0", gathers)
            stream = [G[i].astype(F32) for i in range(8)]
        else:
            arrive(f"gather{l}", gathers)
            attended = jnp.concatenate([A[l - 1, i] for i in range(4)], axis=1)
            out_y[l - 1].done()
            arrive(f"cross_last{l}", crossed_last[l - 1])
            exchanges, parts = [], []
            for half in range(2):
                weight = jnp.concatenate(
                    [WO[l - 1, i, 2 * half : 2 * half + 2].reshape(512, 128) for i in range(4)], axis=1
                )
                part = lax.dot_general(
                    attended, weight, (((1,), (1,)), ((), ())), preferred_element_type=F32
                )
                SX[l - 1, half] = part.astype(BF)
                exchanges.append(rdma(SX.at[l - 1, half], RX.at[l - 1, half], partner))
                parts.append(part)
            stream = []
            for half in range(2):
                arrive(f"exchange{l}_{half}", exchanges[half : half + 1])
                whole = (parts[half] + RX[l - 1, half].astype(F32)).astype(BF).astype(F32)
                stream += [whole[:, i * 128 : (i + 1) * 128] for i in range(4)]
        total = jnp.zeros((128, 1), F32)
        for part in stream:
            total += jnp.sum(part * part, axis=1, keepdims=True)
        scale = lax.rsqrt(total * (1.0 / 1024) + EPS)
        normed = jnp.concatenate(
            [
                (part * scale * gain_ref[l : l + 1, i * 128 : (i + 1) * 128]).astype(BF)
                for i, part in enumerate(stream)
            ],
            axis=1,
        )
        qkv[l].done()
        key_raw = jnp.dot(normed, W[l, 1].reshape(1024, 128), preferred_element_type=F32)
        value_raw = jnp.dot(normed, W[l, 2].reshape(1024, 128), preferred_element_type=F32)
        KV[l, 0, 128:256] = head_norm(key_raw).astype(BF)
        KV[l, 1, 128:256] = value_raw.astype(BF)
        halos = [
            rdma(KV.at[l, :, 128:256], KV.at[l, :, 0:128], nxt),
            rdma(KV.at[l, :, 128:224], KV.at[l, :, 256:352], prv),
        ]
        if l == 0:
            qkv[1].one()
            out_p[0].two()
            out_y[0].two()
        elif l == 1:
            qkv[2].one()
            out_p[1].two()
            out_y[1].two()
        query = head_norm(
            jnp.dot(normed, W[l, 0].reshape(1024, 128), preferred_element_type=F32)
        ).astype(BF)
        query = query * jnp.asarray(0.125, BF)
        zero = jnp.zeros_like(query)
        query = jnp.concatenate([jnp.where(left, query, zero), jnp.where(left, zero, query)], axis=0)
        arrive(f"halo{l}", halos)
        scores = lax.dot_general(
            query, KV[l, 0], (((1,), (1,)), ((), ())), preferred_element_type=F32
        ) + BM[l]
        probs = jnp.exp(scores - jnp.max(scores, axis=1, keepdims=True))
        norm = jnp.sum(probs, axis=1, keepdims=True)
        mixed = jnp.dot(probs.astype(BF), KV[l, 1], preferred_element_type=F32) / norm
        heads = jnp.where(left, mixed[:128], mixed[128:]).astype(BF)
        if l < LAYERS - 1:
            A[l, y] = heads
            gathers = [rdma(A.at[l, y], A.at[l, y], y_peer(d)) for d in RING]
            qkv[l + 1].two()
            out_p[l].done()
            crossed_last[l] = cross_y_last(l)
            if l == 0:
                out_p[1].one()
                arrive("cross1", crossed[1])
                out_y[1].one()
                out_last.one()
            else:
                out_last.two()
            continue
        out_last.done()
        partial = lax.dot_general(
            heads, WL[...].reshape(1024, 128), (((1,), (1,)), ((), ())), preferred_element_type=F32
        ).astype(BF)
        for i in range(8):
            S[i] = partial[:, i * 128 : (i + 1) * 128]
        reduces = []
        for i, (dy, dc) in enumerate(TP_PEERS):
            peer = tp_peer(dy, dc)
            reduces.append(rdma(S.at[peer], R.at[i], {"tp": peer}))
        result = S[t].astype(F32)
        arrive("reduce", reduces)
        for i in range(7):
            result += R[i].astype(F32)
        out_ref[...] = result.astype(BF)

    with jax.named_scope("wait_sends"):
        for copy in sends:
            copy.wait_send()


def local(tokens, norm_gain, w_query, w_key, w_value, w_out, offset_bias, documents):
    vmem = pl.BlockSpec(memory_space=pltpu.VMEM)
    hbm = pl.BlockSpec(memory_space=pl.ANY)
    return pl.pallas_call(
        kernel,
        out_shape=jax.ShapeDtypeStruct((128, 128), BF),
        in_specs=[hbm, vmem, hbm, hbm, hbm, hbm, vmem, hbm],
        out_specs=vmem,
        scratch_shapes=[
            pltpu.VMEM((LAYERS, 3, 4, 4, 64, 128), BF),
            pltpu.VMEM((LAYERS - 1, 4, 4, 4, 64, 128), BF),
            pltpu.VMEM((4, 4, 64, 128), BF),
            pltpu.VMEM((8, 128, 128), BF),
            pltpu.VMEM((LAYERS - 1, 4, 128, 128), BF),
            pltpu.VMEM((LAYERS, 2, 384, 128), BF),
            pltpu.VMEM((3, 1, 128), jnp.int32),
            pltpu.VMEM((7, 128, 128), BF),
            pltpu.VMEM((8, 128, 128), BF),
            pltpu.VMEM((LAYERS - 1, 2, 128, 512), BF),
            pltpu.VMEM((LAYERS - 1, 2, 128, 512), BF),
            pltpu.VMEM((LAYERS, 256, 384), F32),
            pltpu.VMEM((6, 512), F32),
            pltpu.SemaphoreType.DMA((N_COPIES,)),
            pltpu.SemaphoreType.DMA((N_COPIES,)),
            pltpu.SemaphoreType.DMA((7,)),
        ],
        compiler_params=pltpu.CompilerParams(collective_id=0, has_side_effects=True),
    )(
        tokens, norm_gain, w_query, w_key, w_value, jnp.swapaxes(w_out, 1, 2),
        offset_bias.reshape(2 * LAYERS, 8, 16), documents.reshape(1, 128),
    )


def solution(mesh):
    return jax.shard_map(
        local,
        mesh=mesh,
        in_specs=(
            P("sp", "tp"),
            P(),
            P(None, "sp", "tp"),
            P(None, "sp", "tp"),
            P(None, "sp", "tp"),
            P(None, "tp", "sp"),
            P(None, "tp", None, None),
            P("sp"),
        ),
        out_specs=P("sp", "tp"),
        check_vma=False,
    )
```

```python
import math

import jax
import jax.numpy as jnp
from jax import lax
from jax.experimental import pallas as pl
from jax.experimental.pallas import tpu as pltpu
from jax.sharding import PartitionSpec as P

MESH = pl.DeviceIdType.MESH
LAYERS = 3
EPS = 1e-06
NEG = -1e30
BF = jnp.bfloat16
F32 = jnp.float32

RING = (2, 1, 3)
TP_PEERS = ((2, 0), (2, 1), (1, 0), (3, 0), (1, 1), (3, 1), (0, 1))
Y_FIRST = (32, 16)
N_GROUPS = 48
ALL_ROWS = 32768


def kernel(
    tok_ref, gain_ref, wq_ref, wk_ref, wv_ref, wo_ref, bias_ref, docs_ref, out_ref,
    W, WO, WL, G, A, KV, DOC, R, S, RX, SX, BM, PB, ALL, ssem, rsem, lsem,
):
    s = lax.axis_index("sp")
    t = lax.axis_index("tp")
    z, x = s // 4, s % 4
    y, c = t // 2, t % 2
    sent, groups = [], []

    class Group:
        def __init__(self, name, landing):
            self.name, self.landing, self.sem = name, landing, rsem.at[len(groups)]
            groups.append(self)

        def send(self, src, dst, device, send_sem=None):
            if send_sem is None:
                send_sem = ssem.at[0]
                sent.append(math.prod(src.shape) // 128)
            pltpu.make_async_remote_copy(
                src_ref=src,
                dst_ref=dst,
                send_sem=send_sem,
                recv_sem=self.sem,
                device_id=device,
                device_id_type=MESH,
            ).start()

        def wait(self):
            with jax.named_scope(self.name):
                pltpu.make_async_copy(self.landing, self.landing, self.sem).wait()

    def x_peer(d):
        return {"sp": z * 4 + (x + d) % 4}

    def z_peer(d):
        return {"sp": ((z + d) % 4) * 4 + x}

    def y_peer(d):
        return {"tp": ((y + d) % 4) * 2 + c}

    def tp_peer(dy, dc):
        return ((y + dy) % 4) * 2 + (c + dc) % 2

    nxt, prv = {"sp": (s + 1) % 16}, {"sp": (s + 15) % 16}
    partner = {"tp": y * 2 + 1 - c}

    local = [
        pltpu.make_async_copy(tok_ref, G.at[t], lsem.at[0]),
        pltpu.make_async_copy(docs_ref, DOC.at[1], lsem.at[1]),
        pltpu.make_async_copy(wq_ref, W.at[:, 0, z, x], lsem.at[2]),
        pltpu.make_async_copy(wk_ref, W.at[:, 1, z, x], lsem.at[3]),
        pltpu.make_async_copy(wv_ref, W.at[:, 2, z, x], lsem.at[4]),
        pltpu.make_async_copy(wo_ref.at[0:2], WO.at[:, y, z, x], lsem.at[5]),
        pltpu.make_async_copy(wo_ref.at[2], WL.at[z, x], lsem.at[6]),
    ]
    with jax.named_scope("init"):
        for copy in local:
            copy.start()

    barrier = pltpu.get_barrier_semaphore()
    greeted = [x_peer(d) for d in RING] + [z_peer(d) for d in RING] + [nxt, prv]
    greeted += [{"tp": tp_peer(dy, dc)} for dy, dc in TP_PEERS]
    for device in greeted:
        pl.semaphore_signal(barrier, inc=1, device_id=device, device_id_type=MESH)

    PB[...] = jnp.zeros_like(PB)
    for l in range(LAYERS):
        KV[l, :, 352:384, :] = jnp.zeros((2, 32, 128), BF)

    with jax.named_scope("wait_local"):
        for copy in local:
            copy.wait()
    with jax.named_scope("wait_barrier"):
        pl.semaphore_wait(barrier, len(greeted))

    every = slice(None)

    class Plane:
        def __init__(self, name, ref, low, high):
            self.ref = ref
            mid = (low + high) // 16 * 8
            self.a, self.b = slice(low, mid), slice(mid, high)
            rows = slice(low, high)
            self.first = Group("p1_" + name, ref(0, slice(0, 3), rows))
            self.second = Group("p2_" + name, ref(slice(0, 3), every, rows))

        def one(self):
            for d in RING:
                here = self.ref(z, x, self.a)
                self.first.send(here, here, x_peer(d))
                here = self.ref(z, x, self.b)
                self.first.send(here, here, z_peer(d))

        def two(self):
            self.first.wait()
            for d in RING:
                here = self.ref(z, every, self.a)
                self.second.send(here, here, z_peer(d))
                here = self.ref(every, x, self.b)
                self.second.send(here, here, x_peer(d))

        def done(self):
            self.second.wait()

    class Prompt:
        def __init__(self, name, ref):
            self.ref = ref
            self.a, self.b, self.all = slice(0, 32), slice(32, 64), slice(0, 64)
            self.from_x = {d: Group(f"p1x{d}_{name}", ref(0, 0, self.all)) for d in (1, 3, 2)}
            self.from_z = {d: Group(f"p1z{d}_{name}", ref(0, 0, self.all)) for d in (1, 3, 2)}
            self.second = Group("p2_" + name, ref(slice(0, 3), slice(0, 3), self.all))

        def one(self):
            here = self.ref(z, x, self.all)
            for d in (1, 3, 2):
                self.from_x[d].send(here, here, x_peer(d))
                self.from_z[d].send(here, here, z_peer(d))

        def two(self):
            for e in (1, 3, 2):
                self.from_x[e].wait()
                here = self.ref(z, (x - e + 4) % 4, self.a)
                for d in (1, 3, 2):
                    self.second.send(here, here, z_peer(d))
                self.from_z[e].wait()
                here = self.ref((z - e + 4) % 4, x, self.b)
                for d in (1, 3, 2):
                    self.second.send(here, here, x_peer(d))

        def done(self):
            self.second.wait()

    qkv = [
        (Plane if l else Prompt)(
            f"qkv{l}", lambda i, j, rows, l=l: W.at[l, :, i, j, rows], *((0, 64) if l else ())
        )
        for l in range(LAYERS)
    ]
    out_y = [
        Plane(f"oy{l}", lambda i, j, rows, l=l: WO.at[l, :, i, j, rows], 0, Y_FIRST[l])
        for l in range(LAYERS - 1)
    ]
    out_p = [
        Plane(f"op{l}", lambda i, j, rows, l=l: WO.at[l, y, i, j, rows], Y_FIRST[l], 64)
        for l in range(LAYERS - 1)
    ]
    out_last = Plane("ol", lambda i, j, rows: WL.at[i, j, rows], 0, 64)
    cross_first = [
        Group(f"cross{l}", WO.at[l, 0:3, 0, 0, 0 : Y_FIRST[l]]) for l in range(LAYERS - 1)
    ]
    cross_last = [
        Group(f"cross_last{l}", WO.at[l, 0:3, :, :, Y_FIRST[l] : 64]) for l in range(LAYERS - 1)
    ]

    def cross_y_first(l):
        ref = WO.at[l, y, z, x, 0 : Y_FIRST[l]]
        for d in RING:
            cross_first[l].send(ref, ref, y_peer(d))

    def cross_y_last(l):
        out_p[l].done()
        ref = WO.at[l, y, :, :, Y_FIRST[l] : 64]
        for d in RING:
            cross_last[l].send(ref, ref, y_peer(d))

    tokens = Group("gather0", G.at[0:7])
    attended_copies = [Group(f"gather{l + 1}", A.at[l, 0:3]) for l in range(LAYERS - 1)]
    docs = Group("docs", DOC.at[0:2])
    exchanges = [
        [Group(f"exchange{l + 1}_{half}", RX.at[l, half]) for half in range(2)]
        for l in range(LAYERS - 1)
    ]
    halos = [Group(f"halo{l}", KV.at[l, :, 0:224]) for l in range(LAYERS)]
    reduces = Group("reduce", R)

    qkv[0].one()
    for dy, dc in TP_PEERS:
        tokens.send(G.at[t], G.at[t], {"tp": tp_peer(dy, dc)})
    docs.send(DOC.at[1], DOC.at[0], nxt, ssem.at[1])
    docs.send(DOC.at[1], DOC.at[2], prv, ssem.at[1])
    cross_y_first(0)
    out_p[0].one()
    cross_y_first(1)
    out_p[1].one()
    qkv[0].two()
    out_p[0].two()
    cross_first[0].wait()
    out_y[0].one()

    docs.wait()
    qi = lax.broadcasted_iota(jnp.int32, (128, 384), 0)
    kj = lax.broadcasted_iota(jnp.int32, (128, 384), 1)
    row_off = (kj >> 5) - (qi >> 5)
    col_off = (kj & 31) - (qi & 31) + 8
    key_docs = jnp.concatenate([DOC[0], DOC[1], DOC[2]], axis=1)
    eye = lax.broadcasted_iota(jnp.int32, (128, 128), 0) == lax.broadcasted_iota(jnp.int32, (128, 128), 1)
    own_docs = jnp.sum(
        jnp.where(eye, jnp.broadcast_to(DOC[1], (128, 128)).astype(F32), 0.0), axis=1, keepdims=True
    )
    lowest = jnp.where(s > 0, 0, 128)
    highest = jnp.where(s < 15, 384, 256)
    allowed = (
        (row_off >= 0) & (row_off < 8) & (col_off >= 0) & (col_off < 16)
        & (key_docs.astype(F32) == own_docs) & (kj >= lowest) & (kj < highest)
    )
    lines = jnp.zeros((6, 512), F32)
    for a in range(8):
        PB[:, 0:16] = bias_ref[:, a, :]
        lines += pltpu.roll(PB[...], 119 + 32 * a, 1)
    for l in range(LAYERS):
        for h in range(2):
            line = jnp.broadcast_to(lines[l * 2 + h : l * 2 + h + 1], (128, 512))
            table = pltpu.roll(line, 385, 1, stride=1, stride_axis=0)
            BM[l, pl.ds(h * 128, 128), :] = jnp.where(allowed, table[:, :384], NEG)

    lane = lax.broadcasted_iota(jnp.int32, (128, 128), 1)
    left = lane < 64

    def head_norm(raw):
        values = raw.astype(BF).astype(F32)
        squares = values * values
        total0 = jnp.sum(jnp.where(left, squares, 0.0), axis=1, keepdims=True)
        total1 = jnp.sum(jnp.where(left, 0.0, squares), axis=1, keepdims=True)
        mean = jnp.where(left, total0, total1) * (1.0 / 64)
        return values * lax.rsqrt(mean + EPS)

    for l in range(LAYERS):
        if l == 0:
            tokens.wait()
            stream = [G[i].astype(F32) for i in range(8)]
        else:
            attended_copies[l - 1].wait()
            attended = jnp.concatenate([A[l - 1, i] for i in range(4)], axis=1)
            out_y[l - 1].done()
            cross_last[l - 1].wait()
            parts = []
            for half in range(2):
                weight = jnp.concatenate(
                    [WO[l - 1, i, 2 * half : 2 * half + 2].reshape(512, 128) for i in range(4)], axis=1
                )
                part = lax.dot_general(
                    attended, weight, (((1,), (1,)), ((), ())), preferred_element_type=F32
                )
                SX[l - 1, half] = part.astype(BF)
                exchanges[l - 1][half].send(SX.at[l - 1, half], RX.at[l - 1, half], partner)
                parts.append(part)
            if l == 1:
                cross_y_last(1)
            stream = []
            for half in range(2):
                exchanges[l - 1][half].wait()
                whole = (parts[half] + RX[l - 1, half].astype(F32)).astype(BF).astype(F32)
                stream += [whole[:, i * 128 : (i + 1) * 128] for i in range(4)]
        total = jnp.zeros((128, 1), F32)
        for part in stream:
            total += jnp.sum(part * part, axis=1, keepdims=True)
        scale = lax.rsqrt(total * (1.0 / 1024) + EPS)
        normed = jnp.concatenate(
            [
                (part * scale * gain_ref[l : l + 1, i * 128 : (i + 1) * 128]).astype(BF)
                for i, part in enumerate(stream)
            ],
            axis=1,
        )
        qkv[l].done()
        if l == 0:
            cross_y_last(0)
        key_raw = jnp.dot(normed, W[l, 1].reshape(1024, 128), preferred_element_type=F32)
        value_raw = jnp.dot(normed, W[l, 2].reshape(1024, 128), preferred_element_type=F32)
        KV[l, 0, 128:256] = head_norm(key_raw).astype(BF)
        KV[l, 1, 128:256] = value_raw.astype(BF)
        halos[l].send(KV.at[l, :, 128:256], KV.at[l, :, 0:128], nxt)
        halos[l].send(KV.at[l, :, 128:224], KV.at[l, :, 256:352], prv)
        if l == 0:
            qkv[1].one()
            out_y[0].two()
            out_p[1].two()
            cross_first[1].wait()
            out_y[1].one()
        elif l == 1:
            out_y[1].two()
            qkv[2].two()
            out_last.one()
        query = head_norm(
            jnp.dot(normed, W[l, 0].reshape(1024, 128), preferred_element_type=F32)
        ).astype(BF)
        query = query * jnp.asarray(0.125, BF)
        zero = jnp.zeros_like(query)
        query = jnp.concatenate([jnp.where(left, query, zero), jnp.where(left, zero, query)], axis=0)
        halos[l].wait()
        scores = lax.dot_general(
            query, KV[l, 0], (((1,), (1,)), ((), ())), preferred_element_type=F32
        ) + BM[l]
        probs = jnp.exp(scores - jnp.max(scores, axis=1, keepdims=True))
        norm = jnp.sum(probs, axis=1, keepdims=True)
        mixed = jnp.dot(probs.astype(BF), KV[l, 1], preferred_element_type=F32) / norm
        heads = jnp.where(left, mixed[:128], mixed[128:]).astype(BF)
        if l < LAYERS - 1:
            A[l, y] = heads
            for d in RING:
                attended_copies[l].send(A.at[l, y], A.at[l, y], y_peer(d))
            if l == 0:
                qkv[1].two()
                qkv[2].one()
            else:
                out_last.two()
            continue
        out_last.done()
        partial = lax.dot_general(
            heads, WL[...].reshape(1024, 128), (((1,), (1,)), ((), ())), preferred_element_type=F32
        ).astype(BF)
        for i in range(8):
            S[i] = partial[:, i * 128 : (i + 1) * 128]
        for i, (dy, dc) in enumerate(TP_PEERS):
            peer = tp_peer(dy, dc)
            reduces.send(S.at[peer], R.at[i], {"tp": peer})
        result = S[t].astype(F32)
        reduces.wait()
        for i in range(7):
            result += R[i].astype(F32)
        out_ref[...] = result.astype(BF)

    with jax.named_scope("wait_sends"):
        pltpu.make_async_copy(DOC.at[0:2], DOC.at[0:2], ssem.at[1]).wait()
        everything = ALL.at[0 : sum(sent)]
        pltpu.make_async_copy(everything, everything, ssem.at[0]).wait()


def local(tokens, norm_gain, w_query, w_key, w_value, w_out, offset_bias, documents):
    vmem = pl.BlockSpec(memory_space=pltpu.VMEM)
    hbm = pl.BlockSpec(memory_space=pl.ANY)
    return pl.pallas_call(
        kernel,
        out_shape=jax.ShapeDtypeStruct((128, 128), BF),
        in_specs=[hbm, vmem, hbm, hbm, hbm, hbm, vmem, hbm],
        out_specs=vmem,
        scratch_shapes=[
            pltpu.VMEM((LAYERS, 3, 4, 4, 64, 128), BF),
            pltpu.VMEM((LAYERS - 1, 4, 4, 4, 64, 128), BF),
            pltpu.VMEM((4, 4, 64, 128), BF),
            pltpu.VMEM((8, 128, 128), BF),
            pltpu.VMEM((LAYERS - 1, 4, 128, 128), BF),
            pltpu.VMEM((LAYERS, 2, 384, 128), BF),
            pltpu.VMEM((3, 1, 128), jnp.int32),
            pltpu.VMEM((7, 128, 128), BF),
            pltpu.VMEM((8, 128, 128), BF),
            pltpu.VMEM((LAYERS - 1, 2, 128, 512), BF),
            pltpu.VMEM((LAYERS - 1, 2, 128, 512), BF),
            pltpu.VMEM((LAYERS, 256, 384), F32),
            pltpu.VMEM((6, 512), F32),
            pltpu.VMEM((ALL_ROWS, 128), BF),
            pltpu.SemaphoreType.DMA((2,)),
            pltpu.SemaphoreType.DMA((N_GROUPS,)),
            pltpu.SemaphoreType.DMA((7,)),
        ],
        compiler_params=pltpu.CompilerParams(collective_id=0, has_side_effects=True),
    )(
        tokens, norm_gain, w_query, w_key, w_value, jnp.swapaxes(w_out, 1, 2),
        offset_bias.reshape(2 * LAYERS, 8, 16), documents.reshape(1, 128),
    )


def solution(mesh):
    return jax.shard_map(
        local,
        mesh=mesh,
        in_specs=(
            P("sp", "tp"),
            P(),
            P(None, "sp", "tp"),
            P(None, "sp", "tp"),
            P(None, "sp", "tp"),
            P(None, "tp", "sp"),
            P(None, "tp", None, None),
            P("sp"),
        ),
        out_specs=P("sp", "tp"),
        check_vma=False,
    )
```

```python
import math

import jax
import jax.numpy as jnp
from jax import lax
from jax.experimental import pallas as pl
from jax.experimental.pallas import tpu as pltpu
from jax.sharding import PartitionSpec as P

MESH = pl.DeviceIdType.MESH
LAYERS = 3
EPS = 1e-06
NEG = -1e30
BF = jnp.bfloat16
F32 = jnp.float32

RING = (2, 1, 3)
TP_PEERS = ((2, 0), (2, 1), (1, 0), (3, 0), (1, 1), (3, 1), (0, 1))
Y_FIRST = (32, 32)
N_GROUPS = 64
ALL_ROWS = 32768


def kernel(
    tok_ref, gain_ref, wq_ref, wk_ref, wv_ref, wo_ref, bias_ref, docs_ref, out_ref,
    GAIN, BIAS, W, WO, WL, G, A, KV, DOC, R, S, RX, SX, PART, BM, PB, ALL, ssem, rsem, lsem,
):
    s = lax.axis_index("sp")
    t = lax.axis_index("tp")
    z, x = s // 4, s % 4
    y, c = t // 2, t % 2
    sent, groups = [], []

    class Group:
        def __init__(self, name, landing):
            self.name, self.landing, self.sem = name, landing, rsem.at[len(groups)]
            groups.append(self)

        def send(self, src, dst, device, send_sem=None):
            if send_sem is None:
                send_sem = ssem.at[0]
                sent.append(math.prod(src.shape) // 128)
            pltpu.make_async_remote_copy(
                src_ref=src,
                dst_ref=dst,
                send_sem=send_sem,
                recv_sem=self.sem,
                device_id=device,
                device_id_type=MESH,
            ).start()

        def wait(self):
            with jax.named_scope(self.name):
                pltpu.make_async_copy(self.landing, self.landing, self.sem).wait()

    def x_peer(d):
        return {"sp": z * 4 + (x + d) % 4}

    def z_peer(d):
        return {"sp": ((z + d) % 4) * 4 + x}

    def y_peer(d):
        return {"tp": ((y + d) % 4) * 2 + c}

    def tp_peer(dy, dc):
        return ((y + dy) % 4) * 2 + (c + dc) % 2

    nxt, prv = {"sp": (s + 1) % 16}, {"sp": (s + 15) % 16}
    partner = {"tp": y * 2 + 1 - c}

    local = [
        pltpu.make_async_copy(tok_ref, G.at[t], lsem.at[0]),
        pltpu.make_async_copy(docs_ref, DOC.at[1], lsem.at[1]),
        pltpu.make_async_copy(wq_ref, W.at[:, 2, z, x], lsem.at[2]),
        pltpu.make_async_copy(wk_ref, W.at[:, 0, z, x], lsem.at[3]),
        pltpu.make_async_copy(wv_ref, W.at[:, 1, z, x], lsem.at[4]),
        pltpu.make_async_copy(wo_ref.at[0:2], WO.at[:, y, z, x], lsem.at[5]),
        pltpu.make_async_copy(wo_ref.at[2], WL.at[z, x], lsem.at[6]),
        pltpu.make_async_copy(gain_ref, GAIN, lsem.at[7]),
        pltpu.make_async_copy(bias_ref, BIAS, lsem.at[8]),
    ]
    with jax.named_scope("init"):
        for copy in local:
            copy.start()

    barrier = pltpu.get_barrier_semaphore()
    greeted = [x_peer(d) for d in RING] + [z_peer(d) for d in RING] + [nxt, prv]
    greeted += [{"tp": tp_peer(dy, dc)} for dy, dc in TP_PEERS]
    for device in greeted:
        pl.semaphore_signal(barrier, inc=1, device_id=device, device_id_type=MESH)

    PB[...] = jnp.zeros_like(PB)
    for l in range(LAYERS):
        KV[l, :, 352:384, :] = jnp.zeros((2, 32, 128), BF)

    with jax.named_scope("wait_local"):
        for copy in local:
            copy.wait()
    with jax.named_scope("wait_barrier"):
        pl.semaphore_wait(barrier, len(greeted))

    every = slice(None)

    class Plane:
        def __init__(self, name, ref, low, high):
            self.ref = ref
            mid = (low + high) // 16 * 8
            self.a, self.b = slice(low, mid), slice(mid, high)
            rows = slice(low, high)
            self.first = Group("p1_" + name, ref(0, slice(0, 3), rows))
            self.second = Group("p2_" + name, ref(slice(0, 3), every, rows))

        def one(self):
            for d in RING:
                here = self.ref(z, x, self.a)
                self.first.send(here, here, x_peer(d))
                here = self.ref(z, x, self.b)
                self.first.send(here, here, z_peer(d))

        def two(self):
            self.first.wait()
            for d in RING:
                here = self.ref(z, every, self.a)
                self.second.send(here, here, z_peer(d))
                here = self.ref(every, x, self.b)
                self.second.send(here, here, x_peer(d))

        def done(self):
            self.second.wait()

    class Prompt:
        def __init__(self, name, ref):
            self.ref = ref
            self.a, self.b, self.all = slice(0, 32), slice(32, 64), slice(0, 64)
            self.from_x = {d: Group(f"p1x{d}_{name}", ref(0, 0, self.all)) for d in (1, 3, 2)}
            self.from_z = {d: Group(f"p1z{d}_{name}", ref(0, 0, self.all)) for d in (1, 3, 2)}
            self.second = Group("p2_" + name, ref(slice(0, 3), slice(0, 3), self.all))

        def one(self):
            here = self.ref(z, x, self.all)
            for d in (1, 3, 2):
                self.from_x[d].send(here, here, x_peer(d))
                self.from_z[d].send(here, here, z_peer(d))

        def two(self):
            for e in (1, 3, 2):
                self.from_x[e].wait()
                here = self.ref(z, (x - e + 4) % 4, self.a)
                for d in (1, 3, 2):
                    self.second.send(here, here, z_peer(d))
                self.from_z[e].wait()
                here = self.ref((z - e + 4) % 4, x, self.b)
                for d in (1, 3, 2):
                    self.second.send(here, here, x_peer(d))

        def done(self):
            self.second.wait()

    kv = [
        (Plane if l else Prompt)(
            f"kv{l}", lambda i, j, rows, l=l: W.at[l, 0:2, i, j, rows], *((0, 64) if l else ())
        )
        for l in range(LAYERS)
    ]
    wq = [
        Plane(f"q{l}", lambda i, j, rows, l=l: W.at[l, 2, i, j, rows], 0, 64)
        for l in range(LAYERS)
    ]
    out_y = [
        Plane(f"oy{l}", lambda i, j, rows, l=l: WO.at[l, :, i, j, rows], 0, Y_FIRST[l])
        for l in range(LAYERS - 1)
    ]
    out_p = [
        Plane(f"op{l}", lambda i, j, rows, l=l: WO.at[l, y, i, j, rows], Y_FIRST[l], 64)
        for l in range(LAYERS - 1)
    ]
    out_last = Plane("ol", lambda i, j, rows: WL.at[i, j, rows], 0, 64)
    cross_first = [
        Group(f"cross{l}", WO.at[l, 0:3, 0, 0, 0 : Y_FIRST[l]]) for l in range(LAYERS - 1)
    ]
    cross_last = [
        Group(f"cross_last{l}", WO.at[l, 0:3, :, :, Y_FIRST[l] : 64]) for l in range(LAYERS - 1)
    ]

    def cross_y_first(l):
        ref = WO.at[l, y, z, x, 0 : Y_FIRST[l]]
        for d in RING:
            cross_first[l].send(ref, ref, y_peer(d))

    def cross_y_last(l):
        out_p[l].done()
        ref = WO.at[l, y, :, :, Y_FIRST[l] : 64]
        for d in RING:
            cross_last[l].send(ref, ref, y_peer(d))

    tokens = Group("gather0", G.at[0:7])
    attended_copies = [
        {d: Group(f"gather{l + 1}_{d}", A.at[l, 0]) for d in RING} for l in range(LAYERS - 1)
    ]
    docs = Group("docs", DOC.at[0:2])
    exchanges = [
        [Group(f"exchange{l + 1}_{half}", RX.at[l, half]) for half in range(2)]
        for l in range(LAYERS - 1)
    ]
    halos = [Group(f"halo{l}", KV.at[l, :, 0:224]) for l in range(LAYERS)]
    reduces = Group("reduce", R)

    kv[0].one()
    for dy, dc in TP_PEERS:
        tokens.send(G.at[t], G.at[t], {"tp": tp_peer(dy, dc)})
    docs.send(DOC.at[1], DOC.at[0], nxt, ssem.at[1])
    docs.send(DOC.at[1], DOC.at[2], prv, ssem.at[1])
    cross_y_first(0)
    out_p[0].one()
    cross_y_first(1)
    kv[0].two()
    wq[0].one()
    out_p[0].two()
    cross_first[0].wait()
    out_y[0].one()
    out_p[1].one()

    docs.wait()
    qi = lax.broadcasted_iota(jnp.int32, (128, 384), 0)
    kj = lax.broadcasted_iota(jnp.int32, (128, 384), 1)
    row_off = (kj >> 5) - (qi >> 5)
    col_off = (kj & 31) - (qi & 31) + 8
    key_docs = jnp.concatenate([DOC[0], DOC[1], DOC[2]], axis=1)
    eye = lax.broadcasted_iota(jnp.int32, (128, 128), 0) == lax.broadcasted_iota(jnp.int32, (128, 128), 1)
    own_docs = jnp.sum(
        jnp.where(eye, jnp.broadcast_to(DOC[1], (128, 128)).astype(F32), 0.0), axis=1, keepdims=True
    )
    lowest = jnp.where(s > 0, 0, 128)
    highest = jnp.where(s < 15, 384, 256)
    allowed = (
        (row_off >= 0) & (row_off < 8) & (col_off >= 0) & (col_off < 16)
        & (key_docs.astype(F32) == own_docs) & (kj >= lowest) & (kj < highest)
    )
    lines = jnp.zeros((6, 512), F32)
    for a in range(8):
        PB[:, 0:16] = BIAS[:, a, :]
        lines += pltpu.roll(PB[...], 119 + 32 * a, 1)
    for l in range(LAYERS):
        for h in range(2):
            line = jnp.broadcast_to(lines[l * 2 + h : l * 2 + h + 1], (128, 512))
            table = pltpu.roll(line, 385, 1, stride=1, stride_axis=0)
            BM[l, pl.ds(h * 128, 128), :] = jnp.where(allowed, table[:, :384], NEG)

    lane = lax.broadcasted_iota(jnp.int32, (128, 128), 1)
    left = lane < 64

    def head_norm(raw):
        values = raw.astype(BF).astype(F32)
        squares = values * values
        total0 = jnp.sum(jnp.where(left, squares, 0.0), axis=1, keepdims=True)
        total1 = jnp.sum(jnp.where(left, 0.0, squares), axis=1, keepdims=True)
        mean = jnp.where(left, total0, total1) * (1.0 / 64)
        return values * lax.rsqrt(mean + EPS)

    for l in range(LAYERS):
        if l == 0:
            tokens.wait()
            stream = [G[i].astype(F32) for i in range(8)]
        else:
            out_y[l - 1].done()
            cross_last[l - 1].wait()

            def project(slabs, half):
                weight = jnp.concatenate(
                    [WO[l - 1, i, 2 * half : 2 * half + 2].reshape(512, 128) for i in slabs], axis=1
                )
                some = jnp.concatenate([A[l - 1, i] for i in slabs], axis=1)
                return lax.dot_general(
                    some, weight, (((1,), (1,)), ((), ())), preferred_element_type=F32
                )

            attended_copies[l - 1][1].wait()
            early = (y, (y + 3) % 4)
            for half in range(2):
                PART[half] = project(early, half)
            attended_copies[l - 1][3].wait()
            attended_copies[l - 1][2].wait()
            late = ((y + 1) % 4, (y + 2) % 4)
            parts = []
            for half in range(2):
                part = PART[half] + project(late, half)
                SX[l - 1, half] = part.astype(BF)
                exchanges[l - 1][half].send(SX.at[l - 1, half], RX.at[l - 1, half], partner)
                parts.append(part)
            if l == 1:
                cross_y_last(1)
            stream = []
            for half in range(2):
                exchanges[l - 1][half].wait()
                whole = (parts[half] + RX[l - 1, half].astype(F32)).astype(BF).astype(F32)
                stream += [whole[:, i * 128 : (i + 1) * 128] for i in range(4)]
        total = jnp.zeros((128, 1), F32)
        for part in stream:
            total += jnp.sum(part * part, axis=1, keepdims=True)
        scale = lax.rsqrt(total * (1.0 / 1024) + EPS)
        normed = jnp.concatenate(
            [
                (part * scale * GAIN[l : l + 1, i * 128 : (i + 1) * 128]).astype(BF)
                for i, part in enumerate(stream)
            ],
            axis=1,
        )
        kv[l].done()
        key_raw = jnp.dot(normed, W[l, 0].reshape(1024, 128), preferred_element_type=F32)
        value_raw = jnp.dot(normed, W[l, 1].reshape(1024, 128), preferred_element_type=F32)
        KV[l, 0, 128:256] = head_norm(key_raw).astype(BF)
        KV[l, 1, 128:256] = value_raw.astype(BF)
        halos[l].send(KV.at[l, :, 128:256], KV.at[l, :, 0:128], nxt)
        halos[l].send(KV.at[l, :, 128:224], KV.at[l, :, 256:352], prv)
        if l == 0:
            wq[0].two()
            cross_y_last(0)
            kv[1].one()
            wq[1].one()
            out_y[0].two()
            out_p[1].two()
        elif l == 1:
            out_y[1].two()
            kv[2].two()
            wq[2].two()
        else:
            out_last.two()
        wq[l].done()
        query = head_norm(
            jnp.dot(normed, W[l, 2].reshape(1024, 128), preferred_element_type=F32)
        ).astype(BF)
        query = query * jnp.asarray(0.125, BF)
        zero = jnp.zeros_like(query)
        query = jnp.concatenate([jnp.where(left, query, zero), jnp.where(left, zero, query)], axis=0)
        halos[l].wait()
        scores = lax.dot_general(
            query, KV[l, 0], (((1,), (1,)), ((), ())), preferred_element_type=F32
        ) + BM[l]
        probs = jnp.exp(scores - jnp.max(scores, axis=1, keepdims=True))
        norm = jnp.sum(probs, axis=1, keepdims=True)
        mixed = jnp.dot(probs.astype(BF), KV[l, 1], preferred_element_type=F32) / norm
        heads = jnp.where(left, mixed[:128], mixed[128:]).astype(BF)
        if l < LAYERS - 1:
            A[l, y] = heads
            for d in RING:
                attended_copies[l][d].send(A.at[l, y], A.at[l, y], y_peer(d))
            if l == 0:
                kv[1].two()
                wq[1].two()
                cross_first[1].wait()
                kv[2].one()
                out_y[1].one()
                wq[2].one()
                out_last.one()
            continue
        out_last.done()

        def project_last(to):
            weight = WL[to // 2, pl.ds(to % 2 * 2, 2)].reshape(128, 128)
            return lax.dot_general(
                heads, weight, (((1,), (1,)), ((), ())), preferred_element_type=F32
            )

        for i, (dy, dc) in enumerate(TP_PEERS):
            peer = tp_peer(dy, dc)
            S[i] = project_last(peer).astype(BF)
            reduces.send(S.at[i], R.at[i], {"tp": peer})
        result = project_last(t)
        reduces.wait()
        for i in range(7):
            result += R[i].astype(F32)
        out_ref[...] = result.astype(BF)

    with jax.named_scope("wait_sends"):
        pltpu.make_async_copy(DOC.at[0:2], DOC.at[0:2], ssem.at[1]).wait()
        everything = ALL.at[0 : sum(sent)]
        pltpu.make_async_copy(everything, everything, ssem.at[0]).wait()


def local(tokens, norm_gain, w_query, w_key, w_value, w_out, offset_bias, documents):
    vmem = pl.BlockSpec(memory_space=pltpu.VMEM)
    hbm = pl.BlockSpec(memory_space=pl.ANY)
    return pl.pallas_call(
        kernel,
        out_shape=jax.ShapeDtypeStruct((128, 128), BF),
        in_specs=[hbm] * 8,
        out_specs=vmem,
        scratch_shapes=[
            pltpu.VMEM((LAYERS, 1024), F32),
            pltpu.VMEM((2 * LAYERS, 8, 16), F32),
            pltpu.VMEM((LAYERS, 3, 4, 4, 64, 128), BF),
            pltpu.VMEM((LAYERS - 1, 4, 4, 4, 64, 128), BF),
            pltpu.VMEM((4, 4, 64, 128), BF),
            pltpu.VMEM((8, 128, 128), BF),
            pltpu.VMEM((LAYERS - 1, 4, 128, 128), BF),
            pltpu.VMEM((LAYERS, 2, 384, 128), BF),
            pltpu.VMEM((3, 1, 128), jnp.int32),
            pltpu.VMEM((7, 128, 128), BF),
            pltpu.VMEM((7, 128, 128), BF),
            pltpu.VMEM((LAYERS - 1, 2, 128, 512), BF),
            pltpu.VMEM((LAYERS - 1, 2, 128, 512), BF),
            pltpu.VMEM((2, 128, 512), F32),
            pltpu.VMEM((LAYERS, 256, 384), F32),
            pltpu.VMEM((6, 512), F32),
            pltpu.VMEM((ALL_ROWS, 128), BF),
            pltpu.SemaphoreType.DMA((2,)),
            pltpu.SemaphoreType.DMA((N_GROUPS,)),
            pltpu.SemaphoreType.DMA((9,)),
        ],
        compiler_params=pltpu.CompilerParams(collective_id=0, has_side_effects=True),
    )(
        tokens, norm_gain, w_query, w_key, w_value, jnp.swapaxes(w_out, 1, 2),
        offset_bias.reshape(2 * LAYERS, 8, 16), documents.reshape(1, 128),
    )


def solution(mesh):
    return jax.shard_map(
        local,
        mesh=mesh,
        in_specs=(
            P("sp", "tp"),
            P(),
            P(None, "sp", "tp"),
            P(None, "sp", "tp"),
            P(None, "sp", "tp"),
            P(None, "tp", "sp"),
            P(None, "tp", None, None),
            P("sp"),
        ),
        out_specs=P("sp", "tp"),
        check_vma=False,
    )
```

```python
import math

import jax
import jax.numpy as jnp
from jax import lax
from jax.experimental import pallas as pl
from jax.experimental.pallas import tpu as pltpu
from jax.sharding import PartitionSpec as P

MESH = pl.DeviceIdType.MESH
LAYERS = 3
EPS = 1e-06
NEG = -1e30
BF = jnp.bfloat16
F32 = jnp.float32

RING = (2, 1, 3)
TP_PEERS = ((2, 0), (2, 1), (1, 0), (3, 0), (1, 1), (3, 1), (0, 1))
Y_FIRST = (32, 32)
N_GROUPS = 64
ALL_ROWS = 32768


def kernel(
    tok_ref, gain_ref, wq_ref, wk_ref, wv_ref, wo_ref, bias_ref, docs_ref, out_ref,
    GAIN, BIAS, W, WO, WL, G, A, KV, DOC, R, S, RX, SX, PART, BM, PB, ALL, ssem, rsem, lsem,
):
    s = lax.axis_index("sp")
    t = lax.axis_index("tp")
    z, x = s // 4, s % 4
    y, c = t // 2, t % 2
    sent, groups = [], []

    class Group:
        def __init__(self, name, landing):
            self.name, self.landing, self.sem = name, landing, rsem.at[len(groups)]
            groups.append(self)

        def send(self, src, dst, device, send_sem=None):
            if send_sem is None:
                send_sem = ssem.at[0]
                sent.append(math.prod(src.shape) // 128)
            pltpu.make_async_remote_copy(
                src_ref=src,
                dst_ref=dst,
                send_sem=send_sem,
                recv_sem=self.sem,
                device_id=device,
                device_id_type=MESH,
            ).start()

        def wait(self):
            with jax.named_scope(self.name):
                pltpu.make_async_copy(self.landing, self.landing, self.sem).wait()

    def x_peer(d):
        return {"sp": z * 4 + (x + d) % 4}

    def z_peer(d):
        return {"sp": ((z + d) % 4) * 4 + x}

    def y_peer(d):
        return {"tp": ((y + d) % 4) * 2 + c}

    def tp_peer(dy, dc):
        return ((y + dy) % 4) * 2 + (c + dc) % 2

    nxt, prv = {"sp": (s + 1) % 16}, {"sp": (s + 15) % 16}
    partner = {"tp": y * 2 + 1 - c}

    local = [
        pltpu.make_async_copy(tok_ref, G.at[t], lsem.at[0]),
        pltpu.make_async_copy(docs_ref, DOC.at[1], lsem.at[1]),
        pltpu.make_async_copy(wq_ref, W.at[:, 2, z, x], lsem.at[2]),
        pltpu.make_async_copy(wk_ref, W.at[:, 0, z, x], lsem.at[3]),
        pltpu.make_async_copy(wv_ref, W.at[:, 1, z, x], lsem.at[4]),
        pltpu.make_async_copy(wo_ref.at[0:2], WO.at[:, y, z, x], lsem.at[5]),
        pltpu.make_async_copy(wo_ref.at[2], WL.at[z, x], lsem.at[6]),
        pltpu.make_async_copy(gain_ref, GAIN, lsem.at[7]),
        pltpu.make_async_copy(bias_ref, BIAS, lsem.at[8]),
    ]
    with jax.named_scope("init"):
        for copy in local:
            copy.start()

    barrier = pltpu.get_barrier_semaphore()
    greeted = [x_peer(d) for d in RING] + [z_peer(d) for d in RING] + [nxt, prv]
    greeted += [{"tp": tp_peer(dy, dc)} for dy, dc in TP_PEERS]
    for device in greeted:
        pl.semaphore_signal(barrier, inc=1, device_id=device, device_id_type=MESH)

    PB[...] = jnp.zeros_like(PB)
    for l in range(LAYERS):
        KV[l, :, 352:384, :] = jnp.zeros((2, 32, 128), BF)

    with jax.named_scope("wait_local"):
        for copy in local:
            copy.wait()
    with jax.named_scope("wait_barrier"):
        pl.semaphore_wait(barrier, len(greeted))

    every = slice(None)

    class Plane:
        def __init__(self, name, ref, low, high):
            self.ref = ref
            mid = (low + high) // 16 * 8
            self.a, self.b = slice(low, mid), slice(mid, high)
            rows = slice(low, high)
            self.first = Group("p1_" + name, ref(0, slice(0, 3), rows))
            self.second = Group("p2_" + name, ref(slice(0, 3), every, rows))

        def one(self):
            for d in RING:
                here = self.ref(z, x, self.a)
                self.first.send(here, here, x_peer(d))
                here = self.ref(z, x, self.b)
                self.first.send(here, here, z_peer(d))

        def two(self):
            self.first.wait()
            for d in RING:
                here = self.ref(z, every, self.a)
                self.second.send(here, here, z_peer(d))
                here = self.ref(every, x, self.b)
                self.second.send(here, here, x_peer(d))

        def done(self):
            self.second.wait()

    class Prompt:
        def __init__(self, name, ref):
            self.ref = ref
            self.a, self.b, self.all = slice(0, 32), slice(32, 64), slice(0, 64)
            self.from_x = {d: Group(f"p1x{d}_{name}", ref(0, 0, self.all)) for d in (1, 3, 2)}
            self.from_z = {d: Group(f"p1z{d}_{name}", ref(0, 0, self.all)) for d in (1, 3, 2)}
            self.second = Group("p2_" + name, ref(slice(0, 3), slice(0, 3), self.all))

        def one(self):
            here = self.ref(z, x, self.all)
            for d in (1, 3, 2):
                self.from_x[d].send(here, here, x_peer(d))
                self.from_z[d].send(here, here, z_peer(d))

        def two(self):
            for e in (1, 3, 2):
                self.from_x[e].wait()
                here = self.ref(z, (x - e + 4) % 4, self.a)
                for d in (1, 3, 2):
                    self.second.send(here, here, z_peer(d))
                self.from_z[e].wait()
                here = self.ref((z - e + 4) % 4, x, self.b)
                for d in (1, 3, 2):
                    self.second.send(here, here, x_peer(d))

        def done(self):
            self.second.wait()

    kv = [
        (Plane if l else Prompt)(
            f"kv{l}", lambda i, j, rows, l=l: W.at[l, 0:2, i, j, rows], *((0, 64) if l else ())
        )
        for l in range(LAYERS)
    ]
    wq = [
        Plane(f"q{l}", lambda i, j, rows, l=l: W.at[l, 2, i, j, rows], 0, 64)
        for l in range(LAYERS)
    ]
    out_y = [
        Plane(f"oy{l}", lambda i, j, rows, l=l: WO.at[l, :, i, j, rows], 0, Y_FIRST[l])
        for l in range(LAYERS - 1)
    ]
    out_p = [
        Plane(f"op{l}", lambda i, j, rows, l=l: WO.at[l, y, i, j, rows], Y_FIRST[l], 64)
        for l in range(LAYERS - 1)
    ]
    out_last = Plane("ol", lambda i, j, rows: WL.at[i, j, rows], 0, 64)
    cross_first = [
        Group(f"cross{l}", WO.at[l, 0:3, 0, 0, 0 : Y_FIRST[l]]) for l in range(LAYERS - 1)
    ]
    cross_last = [
        Group(f"cross_last{l}", WO.at[l, 0:3, :, :, Y_FIRST[l] : 64]) for l in range(LAYERS - 1)
    ]

    def cross_y_first(l):
        ref = WO.at[l, y, z, x, 0 : Y_FIRST[l]]
        for d in RING:
            cross_first[l].send(ref, ref, y_peer(d))

    def cross_y_last(l):
        out_p[l].done()
        ref = WO.at[l, y, :, :, Y_FIRST[l] : 64]
        for d in RING:
            cross_last[l].send(ref, ref, y_peer(d))

    tokens = Group("gather0", G.at[0:7])
    attended_copies = [
        {d: Group(f"gather{l + 1}_{d}", A.at[l, 0]) for d in RING} for l in range(LAYERS - 1)
    ]
    docs = Group("docs", DOC.at[0:2])
    exchanges = [
        [Group(f"exchange{l + 1}_{half}", RX.at[l, half]) for half in range(2)]
        for l in range(LAYERS - 1)
    ]
    halos = [Group(f"halo{l}", KV.at[l, :, 0:224]) for l in range(LAYERS)]
    reduces = Group("reduce", R)

    kv[0].one()
    for dy, dc in TP_PEERS:
        tokens.send(G.at[t], G.at[t], {"tp": tp_peer(dy, dc)})
    docs.send(DOC.at[1], DOC.at[0], nxt, ssem.at[1])
    docs.send(DOC.at[1], DOC.at[2], prv, ssem.at[1])
    cross_y_first(0)
    out_p[0].one()
    cross_y_first(1)
    kv[0].two()
    wq[0].one()
    out_p[0].two()
    cross_first[0].wait()
    out_y[0].one()

    docs.wait()
    qi = lax.broadcasted_iota(jnp.int32, (128, 384), 0)
    kj = lax.broadcasted_iota(jnp.int32, (128, 384), 1)
    row_off = (kj >> 5) - (qi >> 5)
    col_off = (kj & 31) - (qi & 31) + 8
    key_docs = jnp.concatenate([DOC[0], DOC[1], DOC[2]], axis=1)
    eye = lax.broadcasted_iota(jnp.int32, (128, 128), 0) == lax.broadcasted_iota(jnp.int32, (128, 128), 1)
    own_docs = jnp.sum(
        jnp.where(eye, jnp.broadcast_to(DOC[1], (128, 128)).astype(F32), 0.0), axis=1, keepdims=True
    )
    lowest = jnp.where(s > 0, 0, 128)
    highest = jnp.where(s < 15, 384, 256)
    allowed = (
        (row_off >= 0) & (row_off < 8) & (col_off >= 0) & (col_off < 16)
        & (key_docs.astype(F32) == own_docs) & (kj >= lowest) & (kj < highest)
    )
    lines = jnp.zeros((6, 512), F32)
    for a in range(8):
        PB[:, 0:16] = BIAS[:, a, :]
        lines += pltpu.roll(PB[...], 119 + 32 * a, 1)
    for l in range(LAYERS):
        for h in range(2):
            line = jnp.broadcast_to(lines[l * 2 + h : l * 2 + h + 1], (128, 512))
            table = pltpu.roll(line, 385, 1, stride=1, stride_axis=0)
            BM[l, pl.ds(h * 128, 128), :] = jnp.where(allowed, table[:, :384], NEG)

    lane = lax.broadcasted_iota(jnp.int32, (128, 128), 1)
    left = lane < 64

    def head_norm(raw):
        values = raw.astype(BF).astype(F32)
        squares = values * values
        total0 = jnp.sum(jnp.where(left, squares, 0.0), axis=1, keepdims=True)
        total1 = jnp.sum(jnp.where(left, 0.0, squares), axis=1, keepdims=True)
        mean = jnp.where(left, total0, total1) * (1.0 / 64)
        return values * lax.rsqrt(mean + EPS)

    for l in range(LAYERS):
        if l == 0:
            tokens.wait()
            stream = [G[i].astype(F32) for i in range(8)]
        else:
            out_y[l - 1].done()
            cross_last[l - 1].wait()

            def project(slabs, half):
                weight = jnp.concatenate(
                    [WO[l - 1, i, 2 * half : 2 * half + 2].reshape(512, 128) for i in slabs], axis=1
                )
                some = jnp.concatenate([A[l - 1, i] for i in slabs], axis=1)
                return lax.dot_general(
                    some, weight, (((1,), (1,)), ((), ())), preferred_element_type=F32
                )

            attended_copies[l - 1][1].wait()
            early = (y, (y + 3) % 4)
            for half in range(2):
                PART[half] = project(early, half)
            attended_copies[l - 1][3].wait()
            attended_copies[l - 1][2].wait()
            late = ((y + 1) % 4, (y + 2) % 4)
            parts = []
            for half in range(2):
                part = PART[half] + project(late, half)
                SX[l - 1, half] = part.astype(BF)
                exchanges[l - 1][half].send(SX.at[l - 1, half], RX.at[l - 1, half], partner)
                parts.append(part)
            if l == 1:
                cross_y_last(1)
            stream = []
            for half in range(2):
                exchanges[l - 1][half].wait()
                whole = (parts[half] + RX[l - 1, half].astype(F32)).astype(BF).astype(F32)
                stream += [whole[:, i * 128 : (i + 1) * 128] for i in range(4)]
        squares = stream[0] * stream[0]
        for part in stream[1:]:
            squares += part * part
        total = jnp.sum(squares, axis=1, keepdims=True)
        scale = lax.rsqrt(total * (1.0 / 1024) + EPS)
        normed = jnp.concatenate(
            [
                (part * scale * GAIN[l : l + 1, i * 128 : (i + 1) * 128]).astype(BF)
                for i, part in enumerate(stream)
            ],
            axis=1,
        )
        kv[l].done()
        KV[l, 1, 128:256] = jnp.dot(
            normed, W[l, 1].reshape(1024, 128), preferred_element_type=F32
        ).astype(BF)
        halos[l].send(KV.at[l, 1, 128:256], KV.at[l, 1, 0:128], nxt)
        halos[l].send(KV.at[l, 1, 128:224], KV.at[l, 1, 256:352], prv)
        key_raw = jnp.dot(normed, W[l, 0].reshape(1024, 128), preferred_element_type=F32)
        KV[l, 0, 128:256] = head_norm(key_raw).astype(BF)
        halos[l].send(KV.at[l, 0, 128:256], KV.at[l, 0, 0:128], nxt)
        halos[l].send(KV.at[l, 0, 128:224], KV.at[l, 0, 256:352], prv)
        if l == 0:
            wq[0].two()
            out_p[1].one()
            cross_y_last(0)
            kv[1].one()
            wq[1].one()
            out_y[0].two()
        elif l == 1:
            out_y[1].two()
            kv[2].two()
            wq[2].two()
        wq[l].done()
        query = head_norm(
            jnp.dot(normed, W[l, 2].reshape(1024, 128), preferred_element_type=F32)
        ).astype(BF)
        query = query * jnp.asarray(0.125, BF)
        zero = jnp.zeros_like(query)
        query = jnp.concatenate([jnp.where(left, query, zero), jnp.where(left, zero, query)], axis=0)
        halos[l].wait()
        scores = lax.dot_general(
            query, KV[l, 0], (((1,), (1,)), ((), ())), preferred_element_type=F32
        ) + BM[l]
        probs = jnp.exp(scores)
        norm = jnp.sum(probs, axis=1, keepdims=True)
        mixed = jnp.dot(probs.astype(BF), KV[l, 1], preferred_element_type=F32) / norm
        heads = jnp.where(left, mixed[:128], mixed[128:]).astype(BF)
        if l < LAYERS - 1:
            A[l, y] = heads
            for d in RING:
                attended_copies[l][d].send(A.at[l, y], A.at[l, y], y_peer(d))
            if l == 0:
                out_p[1].two()
                kv[1].two()
                wq[1].two()
                cross_first[1].wait()
                kv[2].one()
                out_y[1].one()
                wq[2].one()
                out_last.one()
            else:
                out_last.two()
            continue
        out_last.done()

        def project_last(to):
            weight = WL[to // 2, pl.ds(to % 2 * 2, 2)].reshape(128, 128)
            return lax.dot_general(
                heads, weight, (((1,), (1,)), ((), ())), preferred_element_type=F32
            )

        for i, (dy, dc) in enumerate(TP_PEERS):
            peer = tp_peer(dy, dc)
            S[i] = project_last(peer).astype(BF)
            reduces.send(S.at[i], R.at[i], {"tp": peer})
        result = project_last(t)
        reduces.wait()
        for i in range(7):
            result += R[i].astype(F32)
        out_ref[...] = result.astype(BF)

    with jax.named_scope("wait_sends"):
        pltpu.make_async_copy(DOC.at[0:2], DOC.at[0:2], ssem.at[1]).wait()
        everything = ALL.at[0 : sum(sent)]
        pltpu.make_async_copy(everything, everything, ssem.at[0]).wait()


def local(tokens, norm_gain, w_query, w_key, w_value, w_out, offset_bias, documents):
    vmem = pl.BlockSpec(memory_space=pltpu.VMEM)
    hbm = pl.BlockSpec(memory_space=pl.ANY)
    return pl.pallas_call(
        kernel,
        out_shape=jax.ShapeDtypeStruct((128, 128), BF),
        in_specs=[hbm] * 8,
        out_specs=vmem,
        scratch_shapes=[
            pltpu.VMEM((LAYERS, 1024), F32),
            pltpu.VMEM((2 * LAYERS, 8, 16), F32),
            pltpu.VMEM((LAYERS, 3, 4, 4, 64, 128), BF),
            pltpu.VMEM((LAYERS - 1, 4, 4, 4, 64, 128), BF),
            pltpu.VMEM((4, 4, 64, 128), BF),
            pltpu.VMEM((8, 128, 128), BF),
            pltpu.VMEM((LAYERS - 1, 4, 128, 128), BF),
            pltpu.VMEM((LAYERS, 2, 384, 128), BF),
            pltpu.VMEM((3, 1, 128), jnp.int32),
            pltpu.VMEM((7, 128, 128), BF),
            pltpu.VMEM((7, 128, 128), BF),
            pltpu.VMEM((LAYERS - 1, 2, 128, 512), BF),
            pltpu.VMEM((LAYERS - 1, 2, 128, 512), BF),
            pltpu.VMEM((2, 128, 512), F32),
            pltpu.VMEM((LAYERS, 256, 384), F32),
            pltpu.VMEM((6, 512), F32),
            pltpu.VMEM((ALL_ROWS, 128), BF),
            pltpu.SemaphoreType.DMA((2,)),
            pltpu.SemaphoreType.DMA((N_GROUPS,)),
            pltpu.SemaphoreType.DMA((9,)),
        ],
        compiler_params=pltpu.CompilerParams(collective_id=0, has_side_effects=True),
    )(
        tokens, norm_gain, w_query, w_key, w_value, jnp.swapaxes(w_out, 1, 2),
        offset_bias.reshape(2 * LAYERS, 8, 16), documents.reshape(1, 128),
    )


def solution(mesh):
    return jax.shard_map(
        local,
        mesh=mesh,
        in_specs=(
            P("sp", "tp"),
            P(),
            P(None, "sp", "tp"),
            P(None, "sp", "tp"),
            P(None, "sp", "tp"),
            P(None, "tp", "sp"),
            P(None, "tp", None, None),
            P("sp"),
        ),
        out_specs=P("sp", "tp"),
        check_vma=False,
    )
```

```python
import math

import jax
import jax.numpy as jnp
from jax import lax
from jax.experimental import pallas as pl
from jax.experimental.pallas import tpu as pltpu
from jax.sharding import PartitionSpec as P

MESH = pl.DeviceIdType.MESH
LAYERS = 3
EPS = 1e-06
NEG = -1e30
BF = jnp.bfloat16
F32 = jnp.float32

RING = (2, 1, 3)
TP_PEERS = ((2, 0), (2, 1), (1, 0), (3, 0), (1, 1), (3, 1), (0, 1))
Y_FIRST = (32, 48)
N_GROUPS = 64
ALL_ROWS = 32768


def kernel(
    tok_ref, gain_ref, wq_ref, wk_ref, wv_ref, wo_ref, bias_ref, docs_ref, out_ref,
    GAIN, BIAS, W, WO, WL, G, A, KV, DOC, R, S, WP, HS, HR, RX, SX, PART, BM, PB, ALL, ssem, rsem, lsem,
):
    s = lax.axis_index("sp")
    t = lax.axis_index("tp")
    z, x = s // 4, s % 4
    y, c = t // 2, t % 2
    sent, groups = [], []

    class Group:
        def __init__(self, name, landing):
            self.name, self.landing, self.sem = name, landing, rsem.at[len(groups)]
            groups.append(self)

        def send(self, src, dst, device, send_sem=None):
            if send_sem is None:
                send_sem = ssem.at[0]
                sent.append(math.prod(src.shape) // 128)
            pltpu.make_async_remote_copy(
                src_ref=src,
                dst_ref=dst,
                send_sem=send_sem,
                recv_sem=self.sem,
                device_id=device,
                device_id_type=MESH,
            ).start()

        def wait(self):
            with jax.named_scope(self.name):
                pltpu.make_async_copy(self.landing, self.landing, self.sem).wait()

    def x_peer(d):
        return {"sp": z * 4 + (x + d) % 4}

    def z_peer(d):
        return {"sp": ((z + d) % 4) * 4 + x}

    def y_peer(d):
        return {"tp": ((y + d) % 4) * 2 + c}

    def tp_peer(dy, dc):
        return ((y + dy) % 4) * 2 + (c + dc) % 2

    nxt, prv = {"sp": (s + 1) % 16}, {"sp": (s + 15) % 16}
    partner = {"tp": y * 2 + 1 - c}

    local = [
        pltpu.make_async_copy(tok_ref, G.at[t], lsem.at[0]),
        pltpu.make_async_copy(docs_ref, DOC.at[1], lsem.at[1]),
        pltpu.make_async_copy(wq_ref, W.at[:, 2, z, x], lsem.at[2]),
        pltpu.make_async_copy(wk_ref, W.at[:, 0, z, x], lsem.at[3]),
        pltpu.make_async_copy(wv_ref, W.at[:, 1, z, x], lsem.at[4]),
        pltpu.make_async_copy(wo_ref.at[0:2], WO.at[:, y, z, x], lsem.at[5]),
        pltpu.make_async_copy(wo_ref.at[2], WL.at[z, x], lsem.at[6]),
        pltpu.make_async_copy(gain_ref, GAIN, lsem.at[7]),
        pltpu.make_async_copy(bias_ref, BIAS, lsem.at[8]),
    ]
    with jax.named_scope("init"):
        for copy in local:
            copy.start()

    barrier = pltpu.get_barrier_semaphore()
    greeted = [x_peer(d) for d in RING] + [z_peer(d) for d in RING] + [nxt, prv]
    greeted += [{"tp": tp_peer(dy, dc)} for dy, dc in TP_PEERS]
    for device in greeted:
        pl.semaphore_signal(barrier, inc=1, device_id=device, device_id_type=MESH)

    PB[...] = jnp.zeros_like(PB)
    for l in range(LAYERS):
        KV[l, :, 352:384, :] = jnp.zeros((2, 32, 128), BF)

    with jax.named_scope("wait_local"):
        for copy in local:
            copy.wait()
    with jax.named_scope("wait_barrier"):
        pl.semaphore_wait(barrier, len(greeted))

    every = slice(None)

    class Plane:
        def __init__(self, name, ref, low, high):
            self.ref = ref
            mid = (low + high) // 16 * 8
            self.a, self.b = slice(low, mid), slice(mid, high)
            rows = slice(low, high)
            self.first = Group("p1_" + name, ref(0, slice(0, 3), rows))
            self.second = Group("p2_" + name, ref(slice(0, 3), every, rows))

        def one(self):
            for d in RING:
                here = self.ref(z, x, self.a)
                self.first.send(here, here, x_peer(d))
                here = self.ref(z, x, self.b)
                self.first.send(here, here, z_peer(d))

        def two(self):
            self.first.wait()
            for d in RING:
                here = self.ref(z, every, self.a)
                self.second.send(here, here, z_peer(d))
                here = self.ref(every, x, self.b)
                self.second.send(here, here, x_peer(d))

        def done(self):
            self.second.wait()

    class Prompt:
        def __init__(self, name, ref):
            self.ref = ref
            self.a, self.b, self.all = slice(0, 32), slice(32, 64), slice(0, 64)
            self.from_x = {d: Group(f"p1x{d}_{name}", ref(0, 0, self.all)) for d in (1, 3, 2)}
            self.from_z = {d: Group(f"p1z{d}_{name}", ref(0, 0, self.all)) for d in (1, 3, 2)}
            self.second = Group("p2_" + name, ref(slice(0, 3), slice(0, 3), self.all))

        def one(self):
            here = self.ref(z, x, self.all)
            for d in (1, 3, 2):
                self.from_x[d].send(here, here, x_peer(d))
                self.from_z[d].send(here, here, z_peer(d))

        def two(self):
            for e in (1, 3, 2):
                self.from_x[e].wait()
                here = self.ref(z, (x - e + 4) % 4, self.a)
                for d in RING:
                    self.second.send(here, here, z_peer(d))
                self.from_z[e].wait()
                here = self.ref((z - e + 4) % 4, x, self.b)
                for d in RING:
                    self.second.send(here, here, x_peer(d))

        def done(self):
            self.second.wait()

    kv = [
        (Plane if l else Prompt)(
            f"kv{l}", lambda i, j, rows, l=l: W.at[l, 0:2, i, j, rows], *((0, 64) if l else ())
        )
        for l in range(LAYERS)
    ]
    wq = [
        Plane(f"q{l}", lambda i, j, rows, l=l: W.at[l, 2, i, j, rows], 0, 64)
        for l in range(LAYERS)
    ]
    out_y = [
        Plane(f"oy{l}", lambda i, j, rows, l=l: WO.at[l, :, i, j, rows], 0, Y_FIRST[l])
        for l in range(LAYERS - 1)
    ]
    out_p = [
        Plane(f"op{l}", lambda i, j, rows, l=l: WO.at[l, y, i, j, rows], Y_FIRST[l], 64)
        for l in range(LAYERS - 1)
    ]
    out_last = Plane("ol", lambda i, j, rows: WL.at[i, j, rows], 0, 64)
    cross_first = [
        Group(f"cross{l}", WO.at[l, 0:3, 0, 0, 0 : Y_FIRST[l]]) for l in range(LAYERS - 1)
    ]
    cross_last = [
        Group(f"cross_last{l}", WO.at[l, 0:3, :, :, Y_FIRST[l] : 64]) for l in range(LAYERS - 1)
    ]

    def cross_y_first(l):
        ref = WO.at[l, y, z, x, 0 : Y_FIRST[l]]
        for d in RING:
            cross_first[l].send(ref, ref, y_peer(d))

    def cross_y_last(l):
        out_p[l].done()
        ref = WO.at[l, y, :, :, Y_FIRST[l] : 64]
        for d in RING:
            cross_last[l].send(ref, ref, y_peer(d))

    tokens = Group("gather0", G.at[0:7])
    attended_copies = [
        {d: Group(f"gather{l + 1}_{d}", A.at[l, 0]) for d in RING} for l in range(LAYERS - 1)
    ]
    docs = Group("docs", DOC.at[0:2])
    exchanges = [
        [Group(f"exchange{l + 1}_{half}", RX.at[l, half]) for half in range(2)]
        for l in range(LAYERS - 1)
    ]
    halos = [Group(f"halo{l}", KV.at[l, :, 0:224]) for l in range(LAYERS)]
    reduces = Group("reduce", R)
    last_weights = Group("last_weights", WP)
    swap = Group("swap", HR)

    kv[0].one()
    for dy, dc in TP_PEERS:
        tokens.send(G.at[t], G.at[t], {"tp": tp_peer(dy, dc)})
    docs.send(DOC.at[1], DOC.at[0], nxt, ssem.at[1])
    docs.send(DOC.at[1], DOC.at[2], prv, ssem.at[1])
    cross_y_first(0)
    out_p[0].one()
    cross_y_first(1)
    kv[0].two()
    wq[0].one()
    out_p[0].two()
    cross_first[0].wait()
    out_y[0].one()

    docs.wait()
    qi = lax.broadcasted_iota(jnp.int32, (128, 384), 0)
    kj = lax.broadcasted_iota(jnp.int32, (128, 384), 1)
    row_off = (kj >> 5) - (qi >> 5)
    col_off = (kj & 31) - (qi & 31) + 8
    key_docs = jnp.concatenate([DOC[0], DOC[1], DOC[2]], axis=1)
    eye = lax.broadcasted_iota(jnp.int32, (128, 128), 0) == lax.broadcasted_iota(jnp.int32, (128, 128), 1)
    own_docs = jnp.sum(
        jnp.where(eye, jnp.broadcast_to(DOC[1], (128, 128)).astype(F32), 0.0), axis=1, keepdims=True
    )
    lowest = jnp.where(s > 0, 0, 128)
    highest = jnp.where(s < 15, 384, 256)
    allowed = (
        (row_off >= 0) & (row_off < 8) & (col_off >= 0) & (col_off < 16)
        & (key_docs.astype(F32) == own_docs) & (kj >= lowest) & (kj < highest)
    )
    lines = jnp.zeros((6, 512), F32)
    for a in range(8):
        PB[:, 0:16] = BIAS[:, a, :]
        lines += pltpu.roll(PB[...], 119 + 32 * a, 1)
    for l in range(LAYERS):
        for h in range(2):
            line = jnp.broadcast_to(lines[l * 2 + h : l * 2 + h + 1], (128, 512))
            table = pltpu.roll(line, 385, 1, stride=1, stride_axis=0)
            BM[l, pl.ds(h * 128, 128), :] = jnp.where(allowed, table[:, :384], NEG)

    lane = lax.broadcasted_iota(jnp.int32, (128, 128), 1)
    left = lane < 64

    def head_norm(raw):
        values = raw.astype(BF).astype(F32)
        squares = values * values
        total0 = jnp.sum(jnp.where(left, squares, 0.0), axis=1, keepdims=True)
        total1 = jnp.sum(jnp.where(left, 0.0, squares), axis=1, keepdims=True)
        mean = jnp.where(left, total0, total1) * (1.0 / 64)
        return values * lax.rsqrt(mean + EPS)

    for l in range(LAYERS):
        if l == 0:
            tokens.wait()
            stream = [G[i].astype(F32) for i in range(8)]
        else:
            out_y[l - 1].done()
            cross_last[l - 1].wait()

            def project(slabs, half):
                weight = jnp.concatenate(
                    [WO[l - 1, i, 2 * half : 2 * half + 2].reshape(512, 128) for i in slabs], axis=1
                )
                some = jnp.concatenate([A[l - 1, i] for i in slabs], axis=1)
                return lax.dot_general(
                    some, weight, (((1,), (1,)), ((), ())), preferred_element_type=F32
                )

            attended_copies[l - 1][1].wait()
            early = (y, (y + 3) % 4)
            for half in range(2):
                PART[half] = project(early, half)
            attended_copies[l - 1][3].wait()
            attended_copies[l - 1][2].wait()
            late = ((y + 1) % 4, (y + 2) % 4)
            parts = []
            for half in range(2):
                part = PART[half] + project(late, half)
                SX[l - 1, half] = part.astype(BF)
                exchanges[l - 1][half].send(SX.at[l - 1, half], RX.at[l - 1, half], partner)
                parts.append(part)
            if l == 1:
                cross_y_last(1)
            stream = []
            for half in range(2):
                exchanges[l - 1][half].wait()
                whole = (parts[half] + RX[l - 1, half].astype(F32)).astype(BF).astype(F32)
                stream += [whole[:, i * 128 : (i + 1) * 128] for i in range(4)]
        squares = stream[0] * stream[0]
        for part in stream[1:]:
            squares += part * part
        total = jnp.sum(squares, axis=1, keepdims=True)
        scale = lax.rsqrt(total * (1.0 / 1024) + EPS)
        normed = jnp.concatenate(
            [
                (part * scale * GAIN[l : l + 1, i * 128 : (i + 1) * 128]).astype(BF)
                for i, part in enumerate(stream)
            ],
            axis=1,
        )
        kv[l].done()
        KV[l, 1, 128:256] = jnp.dot(
            normed, W[l, 1].reshape(1024, 128), preferred_element_type=F32
        ).astype(BF)
        halos[l].send(KV.at[l, 1, 128:256], KV.at[l, 1, 0:128], nxt)
        halos[l].send(KV.at[l, 1, 128:224], KV.at[l, 1, 256:352], prv)
        key_raw = jnp.dot(normed, W[l, 0].reshape(1024, 128), preferred_element_type=F32)
        KV[l, 0, 128:256] = head_norm(key_raw).astype(BF)
        halos[l].send(KV.at[l, 0, 128:256], KV.at[l, 0, 0:128], nxt)
        halos[l].send(KV.at[l, 0, 128:224], KV.at[l, 0, 256:352], prv)
        if l == 0:
            wq[0].two()
            out_p[1].one()
            cross_y_last(0)
            kv[1].one()
            wq[1].one()
            out_y[0].two()
        elif l == 1:
            out_y[1].two()
            kv[2].two()
            wq[2].two()
        else:
            out_last.done()
            last_weights.send(WL.at[:, pl.ds(2 * (1 - c), 2)], WP, partner)
        wq[l].done()
        query = head_norm(
            jnp.dot(normed, W[l, 2].reshape(1024, 128), preferred_element_type=F32)
        ).astype(BF)
        query = query * jnp.asarray(0.125, BF)
        zero = jnp.zeros_like(query)
        query = jnp.concatenate([jnp.where(left, query, zero), jnp.where(left, zero, query)], axis=0)
        halos[l].wait()
        scores = lax.dot_general(
            query, KV[l, 0], (((1,), (1,)), ((), ())), preferred_element_type=F32
        ) + BM[l]
        probs = jnp.exp(scores)
        norm = jnp.sum(probs, axis=1, keepdims=True)
        mixed = jnp.dot(probs.astype(BF), KV[l, 1], preferred_element_type=F32) / norm
        heads = jnp.where(left, mixed[:128], mixed[128:]).astype(BF)
        if l < LAYERS - 1:
            A[l, y] = heads
            for d in RING:
                attended_copies[l][d].send(A.at[l, y], A.at[l, y], y_peer(d))
            if l == 0:
                out_p[1].two()
                kv[1].two()
                wq[1].two()
                cross_first[1].wait()
                kv[2].one()
                out_y[1].one()
                wq[2].one()
                out_last.one()
            else:
                out_last.two()
            continue
        HS[...] = heads
        swap.send(HS, HR, partner)

        def project_last(some, weight):
            return lax.dot_general(
                some, weight.reshape(512, 128), (((1,), (1,)), ((), ())), preferred_element_type=F32
            )

        own = project_last(heads, WL[:, pl.ds(2 * c, 2)])
        last_weights.wait()
        swap.wait()
        own += project_last(HR[...], WP[...])
        for i in range(4):
            S[i] = own[:, i * 128 : (i + 1) * 128].astype(BF)
        for i, d in enumerate(RING):
            reduces.send(S.at[(y + d) % 4], R.at[i], y_peer(d))
        result = S[y].astype(F32)
        reduces.wait()
        for i in range(3):
            result += R[i].astype(F32)
        out_ref[...] = result.astype(BF)

    with jax.named_scope("wait_sends"):
        pltpu.make_async_copy(DOC.at[0:2], DOC.at[0:2], ssem.at[1]).wait()
        everything = ALL.at[0 : sum(sent)]
        pltpu.make_async_copy(everything, everything, ssem.at[0]).wait()


def local(tokens, norm_gain, w_query, w_key, w_value, w_out, offset_bias, documents):
    vmem = pl.BlockSpec(memory_space=pltpu.VMEM)
    hbm = pl.BlockSpec(memory_space=pl.ANY)
    return pl.pallas_call(
        kernel,
        out_shape=jax.ShapeDtypeStruct((128, 128), BF),
        in_specs=[hbm] * 8,
        out_specs=vmem,
        scratch_shapes=[
            pltpu.VMEM((LAYERS, 1024), F32),
            pltpu.VMEM((2 * LAYERS, 8, 16), F32),
            pltpu.VMEM((LAYERS, 3, 4, 4, 64, 128), BF),
            pltpu.VMEM((LAYERS - 1, 4, 4, 4, 64, 128), BF),
            pltpu.VMEM((4, 4, 64, 128), BF),
            pltpu.VMEM((8, 128, 128), BF),
            pltpu.VMEM((LAYERS - 1, 4, 128, 128), BF),
            pltpu.VMEM((LAYERS, 2, 384, 128), BF),
            pltpu.VMEM((3, 1, 128), jnp.int32),
            pltpu.VMEM((3, 128, 128), BF),
            pltpu.VMEM((4, 128, 128), BF),
            pltpu.VMEM((4, 2, 64, 128), BF),
            pltpu.VMEM((128, 128), BF),
            pltpu.VMEM((128, 128), BF),
            pltpu.VMEM((LAYERS - 1, 2, 128, 512), BF),
            pltpu.VMEM((LAYERS - 1, 2, 128, 512), BF),
            pltpu.VMEM((2, 128, 512), F32),
            pltpu.VMEM((LAYERS, 256, 384), F32),
            pltpu.VMEM((6, 512), F32),
            pltpu.VMEM((ALL_ROWS, 128), BF),
            pltpu.SemaphoreType.DMA((2,)),
            pltpu.SemaphoreType.DMA((N_GROUPS,)),
            pltpu.SemaphoreType.DMA((9,)),
        ],
        compiler_params=pltpu.CompilerParams(collective_id=0, has_side_effects=True),
    )(
        tokens, norm_gain, w_query, w_key, w_value, jnp.swapaxes(w_out, 1, 2),
        offset_bias.reshape(2 * LAYERS, 8, 16), documents.reshape(1, 128),
    )


def solution(mesh):
    return jax.shard_map(
        local,
        mesh=mesh,
        in_specs=(
            P("sp", "tp"),
            P(),
            P(None, "sp", "tp"),
            P(None, "sp", "tp"),
            P(None, "sp", "tp"),
            P(None, "tp", "sp"),
            P(None, "tp", None, None),
            P("sp"),
        ),
        out_specs=P("sp", "tp"),
        check_vma=False,
    )
```

```python
import math

import jax
import jax.numpy as jnp
from jax import lax
from jax.experimental import pallas as pl
from jax.experimental.pallas import tpu as pltpu
from jax.sharding import PartitionSpec as P

MESH = pl.DeviceIdType.MESH
LAYERS = 3
EPS = 1e-06
NEG = -1e30
BF = jnp.bfloat16
F32 = jnp.float32

RING = (2, 1, 3)
TP_PEERS = ((2, 0), (2, 1), (1, 0), (3, 0), (1, 1), (3, 1), (0, 1))
Y_FIRST = (32, 32)
N_GROUPS = 64
ALL_ROWS = 32768


def kernel(
    tok_ref, gain_ref, wq_ref, wk_ref, wv_ref, wo_ref, bias_ref, docs_ref, out_ref,
    GAIN, BIAS, W, WO, WL, G, A, KV, DOC, R, S, WP, HS, HR, RX, SX, PART, BM, PB, ALL, ssem, rsem, lsem,
):
    s = lax.axis_index("sp")
    t = lax.axis_index("tp")
    z, x = s // 4, s % 4
    y, c = t // 2, t % 2
    sent, groups = [], []

    class Group:
        def __init__(self, name, landing):
            self.name, self.landing, self.sem = name, landing, rsem.at[len(groups)]
            groups.append(self)

        def send(self, src, dst, device, send_sem=None):
            if send_sem is None:
                send_sem = ssem.at[0]
                sent.append(math.prod(src.shape) // 128)
            pltpu.make_async_remote_copy(
                src_ref=src,
                dst_ref=dst,
                send_sem=send_sem,
                recv_sem=self.sem,
                device_id=device,
                device_id_type=MESH,
            ).start()

        def wait(self):
            with jax.named_scope(self.name):
                pltpu.make_async_copy(self.landing, self.landing, self.sem).wait()

    def x_peer(d):
        return {"sp": z * 4 + (x + d) % 4}

    def z_peer(d):
        return {"sp": ((z + d) % 4) * 4 + x}

    def y_peer(d):
        return {"tp": ((y + d) % 4) * 2 + c}

    def tp_peer(dy, dc):
        return ((y + dy) % 4) * 2 + (c + dc) % 2

    nxt, prv = {"sp": (s + 1) % 16}, {"sp": (s + 15) % 16}
    partner = {"tp": y * 2 + 1 - c}

    local = [
        pltpu.make_async_copy(tok_ref, G.at[t], lsem.at[0]),
        pltpu.make_async_copy(docs_ref, DOC.at[1], lsem.at[1]),
        pltpu.make_async_copy(wq_ref, W.at[:, 2, z, x], lsem.at[2]),
        pltpu.make_async_copy(wk_ref, W.at[:, 0, z, x], lsem.at[3]),
        pltpu.make_async_copy(wv_ref, W.at[:, 1, z, x], lsem.at[4]),
        pltpu.make_async_copy(wo_ref.at[0:2], WO.at[:, y, z, x], lsem.at[5]),
        pltpu.make_async_copy(wo_ref.at[2], WL.at[z, x], lsem.at[6]),
        pltpu.make_async_copy(gain_ref, GAIN, lsem.at[7]),
        pltpu.make_async_copy(bias_ref, BIAS, lsem.at[8]),
    ]
    with jax.named_scope("init"):
        for copy in local:
            copy.start()

    barrier = pltpu.get_barrier_semaphore()
    greeted = [x_peer(d) for d in RING] + [z_peer(d) for d in RING] + [nxt, prv]
    greeted += [{"tp": tp_peer(dy, dc)} for dy, dc in TP_PEERS]
    for device in greeted:
        pl.semaphore_signal(barrier, inc=1, device_id=device, device_id_type=MESH)

    PB[...] = jnp.zeros_like(PB)
    for l in range(LAYERS):
        KV[l, :, 352:384, :] = jnp.zeros((2, 32, 128), BF)

    with jax.named_scope("wait_local"):
        for copy in local:
            copy.wait()
    with jax.named_scope("wait_barrier"):
        pl.semaphore_wait(barrier, len(greeted))

    every = slice(None)

    class Plane:
        def __init__(self, name, ref, low, high):
            self.ref = ref
            mid = (low + high) // 16 * 8
            self.a, self.b = slice(low, mid), slice(mid, high)
            rows = slice(low, high)
            self.first = Group("p1_" + name, ref(0, slice(0, 3), rows))
            self.second = Group("p2_" + name, ref(slice(0, 3), every, rows))

        def one(self):
            for d in RING:
                here = self.ref(z, x, self.a)
                self.first.send(here, here, x_peer(d))
                here = self.ref(z, x, self.b)
                self.first.send(here, here, z_peer(d))

        def two(self):
            self.first.wait()
            for d in RING:
                here = self.ref(z, every, self.a)
                self.second.send(here, here, z_peer(d))
                here = self.ref(every, x, self.b)
                self.second.send(here, here, x_peer(d))

        def done(self):
            self.second.wait()

    class Relay(Plane):
        def __init__(self, name, ref, low, high):
            super().__init__(name, ref, low, high)
            rows = slice(low, high)
            self.near = Group("near_" + name, ref(slice(0, 2), every, rows))
            self.far = Group("far_" + name, ref(0, every, rows))

        def two(self):
            self.first.wait()
            for d in (1, 3):
                here = self.ref(z, every, self.a)
                self.near.send(here, here, z_peer(d))
                here = self.ref(every, x, self.b)
                self.near.send(here, here, x_peer(d))

        def three(self):
            self.near.wait()
            for d, part in ((1, slice(0, 2)), (3, slice(2, 4))):
                here = self.ref((z - d + 4) % 4, part, self.a)
                self.far.send(here, here, z_peer(d))
                here = self.ref(part, (x - d + 4) % 4, self.b)
                self.far.send(here, here, x_peer(d))

        def done(self):
            self.far.wait()

    class Prompt:
        def __init__(self, name, ref):
            self.ref = ref
            self.a, self.b, self.all = slice(0, 32), slice(32, 64), slice(0, 64)
            self.from_x = {d: Group(f"p1x{d}_{name}", ref(0, 0, self.all)) for d in (1, 3, 2)}
            self.from_z = {d: Group(f"p1z{d}_{name}", ref(0, 0, self.all)) for d in (1, 3, 2)}
            self.second = Group("p2_" + name, ref(slice(0, 3), slice(0, 3), self.all))

        def one(self):
            here = self.ref(z, x, self.all)
            for d in (1, 3, 2):
                self.from_x[d].send(here, here, x_peer(d))
                self.from_z[d].send(here, here, z_peer(d))

        def two(self):
            for e in (1, 3, 2):
                self.from_x[e].wait()
                here = self.ref(z, (x - e + 4) % 4, self.a)
                for d in RING:
                    self.second.send(here, here, z_peer(d))
                self.from_z[e].wait()
                here = self.ref((z - e + 4) % 4, x, self.b)
                for d in RING:
                    self.second.send(here, here, x_peer(d))

        def done(self):
            self.second.wait()

    kv = [
        (Relay if l == 1 else Plane if l else Prompt)(
            f"kv{l}", lambda i, j, rows, l=l: W.at[l, 0:2, i, j, rows], *((0, 64) if l else ())
        )
        for l in range(LAYERS)
    ]
    wq = [
        (Relay if l == 1 else Plane)(f"q{l}", lambda i, j, rows, l=l: W.at[l, 2, i, j, rows], 0, 64)
        for l in range(LAYERS)
    ]
    out_y = [
        Plane(f"oy{l}", lambda i, j, rows, l=l: WO.at[l, :, i, j, rows], 0, Y_FIRST[l])
        for l in range(LAYERS - 1)
    ]
    out_p = [
        Plane(f"op{l}", lambda i, j, rows, l=l: WO.at[l, y, i, j, rows], Y_FIRST[l], 64)
        for l in range(LAYERS - 1)
    ]
    out_last = Plane("ol", lambda i, j, rows: WL.at[i, j, rows], 0, 64)
    cross_first = [
        Group(f"cross{l}", WO.at[l, 0:3, 0, 0, 0 : Y_FIRST[l]]) for l in range(LAYERS - 1)
    ]
    cross_last = [
        Group(f"cross_last{l}", WO.at[l, 0:3, :, :, Y_FIRST[l] : 64]) for l in range(LAYERS - 1)
    ]

    def cross_y_first(l):
        ref = WO.at[l, y, z, x, 0 : Y_FIRST[l]]
        for d in RING:
            cross_first[l].send(ref, ref, y_peer(d))

    def cross_y_last(l):
        out_p[l].done()
        ref = WO.at[l, y, :, :, Y_FIRST[l] : 64]
        for d in RING:
            cross_last[l].send(ref, ref, y_peer(d))

    tokens = Group("gather0", G.at[0:7])
    attended_copies = [
        {d: Group(f"gather{l + 1}_{d}", A.at[l, 0]) for d in RING} for l in range(LAYERS - 1)
    ]
    docs = Group("docs", DOC.at[0:2])
    exchanges = [
        [Group(f"exchange{l + 1}_{half}", RX.at[l, half]) for half in range(2)]
        for l in range(LAYERS - 1)
    ]
    halos = [Group(f"halo{l}", KV.at[l, :, 0:224]) for l in range(LAYERS)]
    reduces = Group("reduce", R)
    last_weights = Group("last_weights", WP)
    swap = Group("swap", HR)

    kv[0].one()
    for dy, dc in TP_PEERS:
        tokens.send(G.at[t], G.at[t], {"tp": tp_peer(dy, dc)})
    docs.send(DOC.at[1], DOC.at[0], nxt, ssem.at[1])
    docs.send(DOC.at[1], DOC.at[2], prv, ssem.at[1])
    cross_y_first(0)
    out_p[0].one()
    wq[0].one()
    cross_y_first(1)
    kv[0].two()
    out_p[0].two()
    wq[0].two()
    cross_first[0].wait()
    out_y[0].one()
    out_p[1].one()
    kv[1].one()
    wq[1].one()

    docs.wait()
    qi = lax.broadcasted_iota(jnp.int32, (128, 384), 0)
    kj = lax.broadcasted_iota(jnp.int32, (128, 384), 1)
    row_off = (kj >> 5) - (qi >> 5)
    col_off = (kj & 31) - (qi & 31) + 8
    key_docs = jnp.concatenate([DOC[0], DOC[1], DOC[2]], axis=1)
    eye = lax.broadcasted_iota(jnp.int32, (128, 128), 0) == lax.broadcasted_iota(jnp.int32, (128, 128), 1)
    own_docs = jnp.sum(
        jnp.where(eye, jnp.broadcast_to(DOC[1], (128, 128)).astype(F32), 0.0), axis=1, keepdims=True
    )
    lowest = jnp.where(s > 0, 0, 128)
    highest = jnp.where(s < 15, 384, 256)
    allowed = (
        (row_off >= 0) & (row_off < 8) & (col_off >= 0) & (col_off < 16)
        & (key_docs.astype(F32) == own_docs) & (kj >= lowest) & (kj < highest)
    )
    lines = jnp.zeros((6, 512), F32)
    for a in range(8):
        PB[:, 0:16] = BIAS[:, a, :]
        lines += pltpu.roll(PB[...], 119 + 32 * a, 1)
    for l in range(LAYERS):
        for h in range(2):
            line = jnp.broadcast_to(lines[l * 2 + h : l * 2 + h + 1], (128, 512))
            table = pltpu.roll(line, 385, 1, stride=1, stride_axis=0)
            BM[l, pl.ds(h * 128, 128), :] = jnp.where(allowed, table[:, :384], NEG)

    lane = lax.broadcasted_iota(jnp.int32, (128, 128), 1)
    left = lane < 64

    def head_norm(raw):
        values = raw.astype(BF).astype(F32)
        squares = values * values
        total0 = jnp.sum(jnp.where(left, squares, 0.0), axis=1, keepdims=True)
        total1 = jnp.sum(jnp.where(left, 0.0, squares), axis=1, keepdims=True)
        mean = jnp.where(left, total0, total1) * (1.0 / 64)
        return values * lax.rsqrt(mean + EPS)

    for l in range(LAYERS):
        if l == 0:
            tokens.wait()
            stream = [G[i].astype(F32) for i in range(8)]
        else:
            out_y[l - 1].done()
            cross_last[l - 1].wait()

            def project(slabs, half):
                weight = jnp.concatenate(
                    [WO[l - 1, i, 2 * half : 2 * half + 2].reshape(512, 128) for i in slabs], axis=1
                )
                some = jnp.concatenate([A[l - 1, i] for i in slabs], axis=1)
                return lax.dot_general(
                    some, weight, (((1,), (1,)), ((), ())), preferred_element_type=F32
                )

            attended_copies[l - 1][1].wait()
            early = (y, (y + 3) % 4)
            for half in range(2):
                PART[half] = project(early, half)
            attended_copies[l - 1][3].wait()
            attended_copies[l - 1][2].wait()
            late = ((y + 1) % 4, (y + 2) % 4)
            parts = []
            for half in range(2):
                part = PART[half] + project(late, half)
                SX[l - 1, half] = part.astype(BF)
                exchanges[l - 1][half].send(SX.at[l - 1, half], RX.at[l - 1, half], partner)
                parts.append(part)
            if l == 1:
                cross_y_last(1)
            stream = []
            for half in range(2):
                exchanges[l - 1][half].wait()
                whole = (parts[half] + RX[l - 1, half].astype(F32)).astype(BF).astype(F32)
                stream += [whole[:, i * 128 : (i + 1) * 128] for i in range(4)]
        squares = stream[0] * stream[0]
        for part in stream[1:]:
            squares += part * part
        total = jnp.sum(squares, axis=1, keepdims=True)
        scale = lax.rsqrt(total * (1.0 / 1024) + EPS)
        normed = jnp.concatenate(
            [
                (part * scale * GAIN[l : l + 1, i * 128 : (i + 1) * 128]).astype(BF)
                for i, part in enumerate(stream)
            ],
            axis=1,
        )
        kv[l].done()
        KV[l, 1, 128:256] = jnp.dot(
            normed, W[l, 1].reshape(1024, 128), preferred_element_type=F32
        ).astype(BF)
        halos[l].send(KV.at[l, 1, 128:256], KV.at[l, 1, 0:128], nxt)
        halos[l].send(KV.at[l, 1, 128:224], KV.at[l, 1, 256:352], prv)
        key_raw = jnp.dot(normed, W[l, 0].reshape(1024, 128), preferred_element_type=F32)
        KV[l, 0, 128:256] = head_norm(key_raw).astype(BF)
        halos[l].send(KV.at[l, 0, 128:256], KV.at[l, 0, 0:128], nxt)
        halos[l].send(KV.at[l, 0, 128:224], KV.at[l, 0, 256:352], prv)
        if l == 0:
            cross_y_last(0)
            out_y[0].two()
            out_p[1].two()
            kv[1].two()
            wq[1].two()
        elif l == 1:
            out_y[1].two()
            kv[2].two()
            wq[2].two()
        else:
            out_last.done()
            last_weights.send(WL.at[:, pl.ds(2 * (1 - c), 2)], WP, partner)
        wq[l].done()
        query = head_norm(
            jnp.dot(normed, W[l, 2].reshape(1024, 128), preferred_element_type=F32)
        ).astype(BF)
        query = query * jnp.asarray(0.125, BF)
        zero = jnp.zeros_like(query)
        query = jnp.concatenate([jnp.where(left, query, zero), jnp.where(left, zero, query)], axis=0)
        halos[l].wait()
        scores = lax.dot_general(
            query, KV[l, 0], (((1,), (1,)), ((), ())), preferred_element_type=F32
        ) + BM[l]
        probs = jnp.exp(scores)
        norm = jnp.sum(probs, axis=1, keepdims=True)
        mixed = jnp.dot(probs.astype(BF), KV[l, 1], preferred_element_type=F32) / norm
        heads = jnp.where(left, mixed[:128], mixed[128:]).astype(BF)
        if l < LAYERS - 1:
            A[l, y] = heads
            for d in RING:
                attended_copies[l][d].send(A.at[l, y], A.at[l, y], y_peer(d))
            if l == 0:
                kv[1].three()
                wq[1].three()
                cross_first[1].wait()
                kv[2].one()
                out_y[1].one()
                wq[2].one()
                out_last.one()
            else:
                out_last.two()
            continue
        HS[...] = heads
        swap.send(HS, HR, partner)

        def project_last(some, weight):
            return lax.dot_general(
                some, weight.reshape(512, 128), (((1,), (1,)), ((), ())), preferred_element_type=F32
            )

        own = project_last(heads, WL[:, pl.ds(2 * c, 2)])
        last_weights.wait()
        swap.wait()
        own += project_last(HR[...], WP[...])
        for i in range(4):
            S[i] = own[:, i * 128 : (i + 1) * 128].astype(BF)
        for i, d in enumerate(RING):
            reduces.send(S.at[(y + d) % 4], R.at[i], y_peer(d))
        result = S[y].astype(F32)
        reduces.wait()
        for i in range(3):
            result += R[i].astype(F32)
        out_ref[...] = result.astype(BF)

    with jax.named_scope("wait_sends"):
        pltpu.make_async_copy(DOC.at[0:2], DOC.at[0:2], ssem.at[1]).wait()
        everything = ALL.at[0 : sum(sent)]
        pltpu.make_async_copy(everything, everything, ssem.at[0]).wait()


def local(tokens, norm_gain, w_query, w_key, w_value, w_out, offset_bias, documents):
    vmem = pl.BlockSpec(memory_space=pltpu.VMEM)
    hbm = pl.BlockSpec(memory_space=pl.ANY)
    return pl.pallas_call(
        kernel,
        out_shape=jax.ShapeDtypeStruct((128, 128), BF),
        in_specs=[hbm] * 8,
        out_specs=vmem,
        scratch_shapes=[
            pltpu.VMEM((LAYERS, 1024), F32),
            pltpu.VMEM((2 * LAYERS, 8, 16), F32),
            pltpu.VMEM((LAYERS, 3, 4, 4, 64, 128), BF),
            pltpu.VMEM((LAYERS - 1, 4, 4, 4, 64, 128), BF),
            pltpu.VMEM((4, 4, 64, 128), BF),
            pltpu.VMEM((8, 128, 128), BF),
            pltpu.VMEM((LAYERS - 1, 4, 128, 128), BF),
            pltpu.VMEM((LAYERS, 2, 384, 128), BF),
            pltpu.VMEM((3, 1, 128), jnp.int32),
            pltpu.VMEM((3, 128, 128), BF),
            pltpu.VMEM((4, 128, 128), BF),
            pltpu.VMEM((4, 2, 64, 128), BF),
            pltpu.VMEM((128, 128), BF),
            pltpu.VMEM((128, 128), BF),
            pltpu.VMEM((LAYERS - 1, 2, 128, 512), BF),
            pltpu.VMEM((LAYERS - 1, 2, 128, 512), BF),
            pltpu.VMEM((2, 128, 512), F32),
            pltpu.VMEM((LAYERS, 256, 384), F32),
            pltpu.VMEM((6, 512), F32),
            pltpu.VMEM((ALL_ROWS, 128), BF),
            pltpu.SemaphoreType.DMA((2,)),
            pltpu.SemaphoreType.DMA((N_GROUPS,)),
            pltpu.SemaphoreType.DMA((9,)),
        ],
        compiler_params=pltpu.CompilerParams(collective_id=0, has_side_effects=True),
    )(
        tokens, norm_gain, w_query, w_key, w_value, jnp.swapaxes(w_out, 1, 2),
        offset_bias.reshape(2 * LAYERS, 8, 16), documents.reshape(1, 128),
    )


def solution(mesh):
    return jax.shard_map(
        local,
        mesh=mesh,
        in_specs=(
            P("sp", "tp"),
            P(),
            P(None, "sp", "tp"),
            P(None, "sp", "tp"),
            P(None, "sp", "tp"),
            P(None, "tp", "sp"),
            P(None, "tp", None, None),
            P("sp"),
        ),
        out_specs=P("sp", "tp"),
        check_vma=False,
    )
```

```python
import math

import jax
import jax.numpy as jnp
from jax import lax
from jax.experimental import pallas as pl
from jax.experimental.pallas import tpu as pltpu
from jax.sharding import PartitionSpec as P

MESH = pl.DeviceIdType.MESH
LAYERS = 3
EPS = 1e-06
NEG = -1e30
BF = jnp.bfloat16
F32 = jnp.float32

RING = (2, 1, 3)
TP_PEERS = ((2, 0), (2, 1), (1, 0), (3, 0), (1, 1), (3, 1), (0, 1))
Y_FIRST = (32, 32)
N_GROUPS = 51
ALL_ROWS = 32768


def kernel(
    tok_ref, gain_ref, wq_ref, wk_ref, wv_ref, wo_ref, bias_ref, docs_ref, out_ref,
    GAIN, BIAS, W, WO, WL, G, A, KV, DOC, R, S, WP, HS, HR, RX, SX, PART, BM, PB, ALL, ssem, rsem, lsem,
):
    s = lax.axis_index("sp")
    t = lax.axis_index("tp")
    z, x = s // 4, s % 4
    y, c = t // 2, t % 2
    sent, groups = [], []

    class Group:
        def __init__(self, name, landing):
            self.name, self.landing, self.sem = name, landing, rsem.at[len(groups)]
            groups.append(self)

        def send(self, src, dst, device, send_sem=None):
            if send_sem is None:
                send_sem = ssem.at[0]
                sent.append(math.prod(src.shape) // 128)
            pltpu.make_async_remote_copy(
                src_ref=src,
                dst_ref=dst,
                send_sem=send_sem,
                recv_sem=self.sem,
                device_id=device,
                device_id_type=MESH,
            ).start()

        def wait(self):
            with jax.named_scope(self.name):
                pltpu.make_async_copy(self.landing, self.landing, self.sem).wait()

    def x_peer(d):
        return {"sp": z * 4 + (x + d) % 4}

    def z_peer(d):
        return {"sp": ((z + d) % 4) * 4 + x}

    def y_peer(d):
        return {"tp": ((y + d) % 4) * 2 + c}

    def tp_peer(dy, dc):
        return ((y + dy) % 4) * 2 + (c + dc) % 2

    nxt, prv = {"sp": (s + 1) % 16}, {"sp": (s + 15) % 16}
    partner = {"tp": y * 2 + 1 - c}

    local = [
        pltpu.make_async_copy(tok_ref, G.at[t], lsem.at[0]),
        pltpu.make_async_copy(docs_ref, DOC.at[1], lsem.at[1]),
        pltpu.make_async_copy(wq_ref, W.at[:, 2, z, x], lsem.at[2]),
        pltpu.make_async_copy(wk_ref, W.at[:, 0, z, x], lsem.at[3]),
        pltpu.make_async_copy(wv_ref, W.at[:, 1, z, x], lsem.at[4]),
        pltpu.make_async_copy(wo_ref.at[0:2], WO.at[:, y, z, x], lsem.at[5]),
        pltpu.make_async_copy(wo_ref.at[2], WL.at[z, x], lsem.at[6]),
        pltpu.make_async_copy(gain_ref, GAIN, lsem.at[7]),
        pltpu.make_async_copy(bias_ref, BIAS, lsem.at[8]),
    ]
    with jax.named_scope("init"):
        for copy in local:
            copy.start()

    barrier = pltpu.get_barrier_semaphore()
    greeted = [x_peer(d) for d in RING] + [z_peer(d) for d in RING] + [nxt, prv]
    greeted += [{"tp": tp_peer(dy, dc)} for dy, dc in TP_PEERS]
    for device in greeted:
        pl.semaphore_signal(barrier, inc=1, device_id=device, device_id_type=MESH)

    PB[...] = jnp.zeros_like(PB)
    for l in range(LAYERS):
        KV[l, :, 352:384, :] = jnp.zeros((2, 32, 128), BF)

    with jax.named_scope("wait_local"):
        for copy in local:
            copy.wait()
    with jax.named_scope("wait_barrier"):
        pl.semaphore_wait(barrier, len(greeted))

    every = slice(None)

    class Plane:
        def __init__(self, name, ref, low, high):
            self.ref = ref
            mid = (low + high) // 16 * 8
            self.a, self.b = slice(low, mid), slice(mid, high)
            rows = slice(low, high)
            self.first = Group("p1_" + name, ref(0, slice(0, 3), rows))
            self.landing(name, rows)

        def landing(self, name, rows):
            self.second = Group("p2_" + name, self.ref(slice(0, 3), every, rows))

        def one(self):
            for d in RING:
                here = self.ref(z, x, self.a)
                self.first.send(here, here, x_peer(d))
                here = self.ref(z, x, self.b)
                self.first.send(here, here, z_peer(d))

        def two(self):
            self.first.wait()
            for d in RING:
                here = self.ref(z, every, self.a)
                self.second.send(here, here, z_peer(d))
                here = self.ref(every, x, self.b)
                self.second.send(here, here, x_peer(d))

        def done(self):
            self.second.wait()

    class Relay(Plane):
        def landing(self, name, rows):
            self.near = Group("near_" + name, self.ref(slice(0, 2), every, rows))
            self.far = Group("far_" + name, self.ref(0, every, rows))

        def two(self):
            self.first.wait()
            for d in (1, 3):
                here = self.ref(z, every, self.a)
                self.near.send(here, here, z_peer(d))
                here = self.ref(every, x, self.b)
                self.near.send(here, here, x_peer(d))

        def three(self):
            self.near.wait()
            for d, part in ((1, slice(0, 2)), (3, slice(2, 4))):
                here = self.ref((z - d + 4) % 4, part, self.a)
                self.far.send(here, here, z_peer(d))
                here = self.ref(part, (x - d + 4) % 4, self.b)
                self.far.send(here, here, x_peer(d))

        def done(self):
            self.far.wait()

    class Prompt:
        def __init__(self, name, ref):
            self.ref = ref
            self.a, self.b, self.all = slice(0, 32), slice(32, 64), slice(0, 64)
            self.from_x = {d: Group(f"p1x{d}_{name}", ref(0, 0, self.all)) for d in (1, 3, 2)}
            self.from_z = {d: Group(f"p1z{d}_{name}", ref(0, 0, self.all)) for d in (1, 3, 2)}
            self.second = Group("p2_" + name, ref(slice(0, 3), slice(0, 3), self.all))

        def one(self):
            here = self.ref(z, x, self.all)
            for d in (1, 3, 2):
                self.from_x[d].send(here, here, x_peer(d))
                self.from_z[d].send(here, here, z_peer(d))

        def two(self):
            for e in (1, 3, 2):
                self.from_x[e].wait()
                here = self.ref(z, (x - e + 4) % 4, self.a)
                for d in RING:
                    self.second.send(here, here, z_peer(d))
                self.from_z[e].wait()
                here = self.ref((z - e + 4) % 4, x, self.b)
                for d in RING:
                    self.second.send(here, here, x_peer(d))

        def done(self):
            self.second.wait()

    kv = [
        (Relay if l == 1 else Plane if l else Prompt)(
            f"kv{l}", lambda i, j, rows, l=l: W.at[l, 0:2, i, j, rows], *((0, 64) if l else ())
        )
        for l in range(LAYERS)
    ]
    wq = [
        (Relay if l == 1 else Plane)(f"q{l}", lambda i, j, rows, l=l: W.at[l, 2, i, j, rows], 0, 64)
        for l in range(LAYERS)
    ]
    out_y = [
        Plane(f"oy{l}", lambda i, j, rows, l=l: WO.at[l, :, i, j, rows], 0, Y_FIRST[l])
        for l in range(LAYERS - 1)
    ]
    out_p = [
        Plane(f"op{l}", lambda i, j, rows, l=l: WO.at[l, y, i, j, rows], Y_FIRST[l], 64)
        for l in range(LAYERS - 1)
    ]
    out_last = Plane("ol", lambda i, j, rows: WL.at[i, j, rows], 0, 64)
    cross_first = [
        Group(f"cross{l}", WO.at[l, 0:3, 0, 0, 0 : Y_FIRST[l]]) for l in range(LAYERS - 1)
    ]
    cross_last = [
        Group(f"cross_last{l}", WO.at[l, 0:3, :, :, Y_FIRST[l] : 64]) for l in range(LAYERS - 1)
    ]

    def cross_y_first(l):
        ref = WO.at[l, y, z, x, 0 : Y_FIRST[l]]
        for d in RING:
            cross_first[l].send(ref, ref, y_peer(d))

    def cross_y_last(l):
        out_p[l].done()
        ref = WO.at[l, y, :, :, Y_FIRST[l] : 64]
        for d in RING:
            cross_last[l].send(ref, ref, y_peer(d))

    tokens = Group("gather0", G.at[0:7])
    attended_copies = [
        {d: Group(f"gather{l + 1}_{d}", A.at[l, 0]) for d in RING} for l in range(LAYERS - 1)
    ]
    docs = Group("docs", DOC.at[0:2])
    exchanges = [
        [Group(f"exchange{l + 1}_{half}", RX.at[l, half]) for half in range(2)]
        for l in range(LAYERS - 1)
    ]
    halos = [Group(f"halo{l}", KV.at[l, :, 0:224]) for l in range(LAYERS)]
    reduces = Group("reduce", R)
    last_weights = Group("last_weights", WP)
    swap = Group("swap", HR)

    kv[0].one()
    for dy, dc in TP_PEERS:
        tokens.send(G.at[t], G.at[t], {"tp": tp_peer(dy, dc)})
    docs.send(DOC.at[1], DOC.at[0], nxt, ssem.at[1])
    docs.send(DOC.at[1], DOC.at[2], prv, ssem.at[1])
    cross_y_first(0)
    out_p[0].one()
    wq[0].one()
    cross_y_first(1)
    kv[0].two()
    out_p[0].two()
    wq[0].two()
    cross_first[0].wait()
    out_y[0].one()
    out_p[1].one()
    kv[1].one()
    wq[1].one()

    docs.wait()
    qi = lax.broadcasted_iota(jnp.int32, (128, 384), 0)
    kj = lax.broadcasted_iota(jnp.int32, (128, 384), 1)
    row_off = (kj >> 5) - (qi >> 5)
    col_off = (kj & 31) - (qi & 31) + 8
    key_docs = jnp.concatenate([DOC[0], DOC[1], DOC[2]], axis=1)
    eye = lax.broadcasted_iota(jnp.int32, (128, 128), 0) == lax.broadcasted_iota(jnp.int32, (128, 128), 1)
    own_docs = jnp.sum(
        jnp.where(eye, jnp.broadcast_to(DOC[1], (128, 128)).astype(F32), 0.0), axis=1, keepdims=True
    )
    lowest = jnp.where(s > 0, 0, 128)
    highest = jnp.where(s < 15, 384, 256)
    allowed = (
        (row_off >= 0) & (row_off < 8) & (col_off >= 0) & (col_off < 16)
        & (key_docs.astype(F32) == own_docs) & (kj >= lowest) & (kj < highest)
    )
    lines = jnp.zeros((6, 512), F32)
    for a in range(8):
        PB[:, 0:16] = BIAS[:, a, :]
        lines += pltpu.roll(PB[...], 119 + 32 * a, 1)
    for l in range(LAYERS):
        for h in range(2):
            line = jnp.broadcast_to(lines[l * 2 + h : l * 2 + h + 1], (128, 512))
            table = pltpu.roll(line, 385, 1, stride=1, stride_axis=0)
            BM[l, pl.ds(h * 128, 128), :] = jnp.where(allowed, table[:, :384], NEG)

    lane = lax.broadcasted_iota(jnp.int32, (128, 128), 1)
    left = lane < 64

    def head_norm(raw):
        values = raw.astype(BF).astype(F32)
        squares = values * values
        total0 = jnp.sum(jnp.where(left, squares, 0.0), axis=1, keepdims=True)
        total1 = jnp.sum(jnp.where(left, 0.0, squares), axis=1, keepdims=True)
        mean = jnp.where(left, total0, total1) * (1.0 / 64)
        return values * lax.rsqrt(mean + EPS)

    for l in range(LAYERS):
        if l == 0:
            tokens.wait()
            stream = [G[i].astype(F32) for i in range(8)]
        else:
            out_y[l - 1].done()
            cross_last[l - 1].wait()

            def project(slabs, half):
                weight = jnp.concatenate(
                    [WO[l - 1, i, 2 * half : 2 * half + 2].reshape(512, 128) for i in slabs], axis=1
                )
                some = jnp.concatenate([A[l - 1, i] for i in slabs], axis=1)
                return lax.dot_general(
                    some, weight, (((1,), (1,)), ((), ())), preferred_element_type=F32
                )

            attended_copies[l - 1][1].wait()
            early = (y, (y + 3) % 4)
            for half in range(2):
                PART[half] = project(early, half)
            attended_copies[l - 1][3].wait()
            attended_copies[l - 1][2].wait()
            late = ((y + 1) % 4, (y + 2) % 4)
            parts = []
            for half in range(2):
                part = PART[half] + project(late, half)
                SX[l - 1, half] = part.astype(BF)
                exchanges[l - 1][half].send(SX.at[l - 1, half], RX.at[l - 1, half], partner)
                parts.append(part)
            if l == 1:
                cross_y_last(1)
            stream = []
            for half in range(2):
                exchanges[l - 1][half].wait()
                whole = (parts[half] + RX[l - 1, half].astype(F32)).astype(BF).astype(F32)
                stream += [whole[:, i * 128 : (i + 1) * 128] for i in range(4)]
        squares = stream[0] * stream[0]
        for part in stream[1:]:
            squares += part * part
        total = jnp.sum(squares, axis=1, keepdims=True)
        scale = lax.rsqrt(total * (1.0 / 1024) + EPS)
        normed = jnp.concatenate(
            [
                (part * scale * GAIN[l : l + 1, i * 128 : (i + 1) * 128]).astype(BF)
                for i, part in enumerate(stream)
            ],
            axis=1,
        )
        kv[l].done()
        KV[l, 1, 128:256] = jnp.dot(
            normed, W[l, 1].reshape(1024, 128), preferred_element_type=F32
        ).astype(BF)
        halos[l].send(KV.at[l, 1, 128:256], KV.at[l, 1, 0:128], nxt)
        halos[l].send(KV.at[l, 1, 128:224], KV.at[l, 1, 256:352], prv)
        key_raw = jnp.dot(normed, W[l, 0].reshape(1024, 128), preferred_element_type=F32)
        KV[l, 0, 128:256] = head_norm(key_raw).astype(BF)
        halos[l].send(KV.at[l, 0, 128:256], KV.at[l, 0, 0:128], nxt)
        halos[l].send(KV.at[l, 0, 128:224], KV.at[l, 0, 256:352], prv)
        if l == 0:
            cross_y_last(0)
            out_y[0].two()
            out_p[1].two()
            kv[1].two()
            wq[1].two()
        elif l == 1:
            out_y[1].two()
            kv[2].two()
            wq[2].two()
        else:
            out_last.done()
            last_weights.send(WL.at[:, pl.ds(2 * (1 - c), 2)], WP, partner)
        wq[l].done()
        query = head_norm(
            jnp.dot(normed, W[l, 2].reshape(1024, 128), preferred_element_type=F32)
        ).astype(BF)
        query = query * jnp.asarray(0.125, BF)
        zero = jnp.zeros_like(query)
        query = jnp.concatenate([jnp.where(left, query, zero), jnp.where(left, zero, query)], axis=0)
        halos[l].wait()
        scores = lax.dot_general(
            query, KV[l, 0], (((1,), (1,)), ((), ())), preferred_element_type=F32
        ) + BM[l]
        probs = jnp.exp(scores)
        norm = jnp.sum(probs, axis=1, keepdims=True)
        mixed = jnp.dot(probs.astype(BF), KV[l, 1], preferred_element_type=F32)
        heads = jnp.where(left, mixed[:128], mixed[128:]) / jnp.where(left, norm[:128], norm[128:])
        heads = heads.astype(BF)
        if l < LAYERS - 1:
            A[l, y] = heads
            for d in RING:
                attended_copies[l][d].send(A.at[l, y], A.at[l, y], y_peer(d))
            if l == 0:
                kv[1].three()
                wq[1].three()
                cross_first[1].wait()
                kv[2].one()
                out_y[1].one()
                wq[2].one()
                out_last.one()
            else:
                out_last.two()
            continue
        HS[...] = heads
        swap.send(HS, HR, partner)

        def project_last(some, weight):
            return lax.dot_general(
                some, weight.reshape(512, 128), (((1,), (1,)), ((), ())), preferred_element_type=F32
            )

        own = project_last(heads, WL[:, pl.ds(2 * c, 2)])
        last_weights.wait()
        swap.wait()
        own += project_last(HR[...], WP[...])
        for i in range(4):
            S[i] = own[:, i * 128 : (i + 1) * 128].astype(BF)
        for i, d in enumerate(RING):
            reduces.send(S.at[(y + d) % 4], R.at[i], y_peer(d))
        result = S[y].astype(F32)
        reduces.wait()
        for i in range(3):
            result += R[i].astype(F32)
        out_ref[...] = result.astype(BF)

    with jax.named_scope("wait_sends"):
        pltpu.make_async_copy(DOC.at[0:2], DOC.at[0:2], ssem.at[1]).wait()
        everything = ALL.at[0 : sum(sent)]
        pltpu.make_async_copy(everything, everything, ssem.at[0]).wait()


def local(tokens, norm_gain, w_query, w_key, w_value, w_out, offset_bias, documents):
    vmem = pl.BlockSpec(memory_space=pltpu.VMEM)
    hbm = pl.BlockSpec(memory_space=pl.ANY)
    return pl.pallas_call(
        kernel,
        out_shape=jax.ShapeDtypeStruct((128, 128), BF),
        in_specs=[hbm] * 8,
        out_specs=vmem,
        scratch_shapes=[
            pltpu.VMEM((LAYERS, 1024), F32),
            pltpu.VMEM((2 * LAYERS, 8, 16), F32),
            pltpu.VMEM((LAYERS, 3, 4, 4, 64, 128), BF),
            pltpu.VMEM((LAYERS - 1, 4, 4, 4, 64, 128), BF),
            pltpu.VMEM((4, 4, 64, 128), BF),
            pltpu.VMEM((8, 128, 128), BF),
            pltpu.VMEM((LAYERS - 1, 4, 128, 128), BF),
            pltpu.VMEM((LAYERS, 2, 384, 128), BF),
            pltpu.VMEM((3, 1, 128), jnp.int32),
            pltpu.VMEM((3, 128, 128), BF),
            pltpu.VMEM((4, 128, 128), BF),
            pltpu.VMEM((4, 2, 64, 128), BF),
            pltpu.VMEM((128, 128), BF),
            pltpu.VMEM((128, 128), BF),
            pltpu.VMEM((LAYERS - 1, 2, 128, 512), BF),
            pltpu.VMEM((LAYERS - 1, 2, 128, 512), BF),
            pltpu.VMEM((2, 128, 512), F32),
            pltpu.VMEM((LAYERS, 256, 384), F32),
            pltpu.VMEM((6, 512), F32),
            pltpu.VMEM((ALL_ROWS, 128), BF),
            pltpu.SemaphoreType.DMA((2,)),
            pltpu.SemaphoreType.DMA((N_GROUPS,)),
            pltpu.SemaphoreType.DMA((9,)),
        ],
        compiler_params=pltpu.CompilerParams(collective_id=0, has_side_effects=True),
    )(
        tokens, norm_gain, w_query, w_key, w_value, jnp.swapaxes(w_out, 1, 2),
        offset_bias.reshape(2 * LAYERS, 8, 16), documents.reshape(1, 128),
    )


def solution(mesh):
    return jax.shard_map(
        local,
        mesh=mesh,
        in_specs=(
            P("sp", "tp"),
            P(),
            P(None, "sp", "tp"),
            P(None, "sp", "tp"),
            P(None, "sp", "tp"),
            P(None, "tp", "sp"),
            P(None, "tp", None, None),
            P("sp"),
        ),
        out_specs=P("sp", "tp"),
        check_vma=False,
    )
```
